32 devices in a mesh: sp: 16 (over z, y, x), tp: 2 (over core).
Axes of the slice: x: 2, y: 2, z: 4, core: 2. Of those that a mesh axis runs over, the one named last changes fastest.
Arguments:
- residual_in: bfloat16 [4096, 2048], P(('sp', 'tp')), may hold values from -6 to 6
- query_lean: bfloat16 [4096, 8, 96], P('sp', 'tp'), may hold values from -60 to 60
- query_broad: bfloat16 [4096, 8, 160], P('sp', 'tp'), may hold values from -60 to 60
- latent: bfloat16 [4096, 256], P('sp'), may hold values from -6 to 6
- rope_key: bfloat16 [4096, 32], P('sp'), may hold values from -8 to 8
- latent_gain: float32 [256], replicated, may hold values from 0.1 to 1.9
- key_up_lean: bfloat16 [256, 8, 64], P(None, 'tp'), may hold values from -0.375 to 0.375
- key_up_broad: bfloat16 [256, 8, 128], P(None, 'tp'), may hold values from -0.375 to 0.375
- value_up_lean: bfloat16 [256, 8, 64], P(None, 'tp'), may hold values from -0.375 to 0.375
- value_up_broad: bfloat16 [256, 8, 128], P(None, 'tp'), may hold values from -0.375 to 0.375
- out_lean: bfloat16 [8, 64, 2048], P('tp'), may hold values from -0.15625 to 0.15625
- out_broad: bfloat16 [8, 128, 2048], P('tp'), may hold values from -0.15625 to 0.15625
- attn_gain: float32 [2048], replicated, may hold values from 0.1 to 1.9
- mlp_gain: float32 [2048], replicated, may hold values from 0.1 to 1.9
- gate_weight: bfloat16 [2048, 2816], P('sp', 'tp'), may hold values from -0.125 to 0.125
- up_weight: bfloat16 [2048, 2816], P('sp', 'tp'), may hold values from -0.125 to 0.125
- down_weight: bfloat16 [2816, 2048], P('tp', 'sp'), may hold values from -0.109375 to 0.109375
Outputs:
- layer_out: bfloat16 [4096, 2048], P(('sp', 'tp'))
The draws below stay inside these ranges and needn't reach their ends.
All inputs are finite; a program needn't handle non-finite values.
Results may differ from the reference program's by a relative error of at most 0.015.
Values may be sent and summed in bfloat16 or wider, within the bound.
A program may use at most 128 MiB of HBM per device.

```python
import math
import jax
import jax.numpy as jnp
from jax import lax

D = 2048
HEADS_A = 8
HEADS_B = 8
NOPE_A = 64
V_A = 64
NOPE_B = 128
V_B = 128
ROPE = 32
KV_RANK = 256
FF = 2816
QK_A = 96
QK_B = 160
TOKENS = 4096
N_TP = 2


def draw_rope_key(key, part):
    base = jax.random.truncated_normal(jax.random.fold_in(key, 1), -4.0, 4.0, (TOKENS, ROPE), jnp.float32)
    return base.astype(jnp.bfloat16)


def draw_query_lean(key, part):
    base = jax.random.truncated_normal(jax.random.fold_in(key, 2), -4.0, 4.0, (TOKENS, HEADS_A, QK_A), jnp.float32)
    return base.astype(jnp.bfloat16)


def draw_query_broad(key, part):
    base = jax.random.truncated_normal(jax.random.fold_in(key, 3), -4.0, 4.0, (TOKENS, HEADS_B, QK_B), jnp.float32)
    return base.astype(jnp.bfloat16)


def levels(key, extent, pieces, smallest, high):
    def one(position, shards_of):
        heights = jax.random.uniform(jax.random.fold_in(jax.random.fold_in(key, 6), position), (shards_of,), jnp.float32, smallest / len(pieces), high / len(pieces))
        return jnp.repeat(jnp.exp(heights), extent[position] // shards_of).reshape((-1,) + (1,) * (len(extent) - position - 1))

    factor_of = one(*pieces[0])
    for cut in pieces[1:]:
        factor_of = factor_of * one(*cut)
    return factor_of


def centred(own_key, extent, scale, bound, cuts=(), held_as=jnp.bfloat16):
    loudness = levels(own_key, extent, cuts, -0.22, 0.18) if cuts else 1.0
    values = jax.random.normal(own_key, extent, jnp.float32) * scale * loudness
    return jnp.minimum(jnp.maximum(values, -bound), bound).astype(held_as)


def setup_inputs(seed: int = 0) -> dict:
    seeds = jax.random.split(jax.random.key(seed), 18)
    return {
        "residual_in": centred(seeds[0], (TOKENS, D), 1.0, 6.0, ((0, 32),)),
        "query_lean": draw_query_lean(jax.random.fold_in(seeds[17], 71), 0),
        "query_broad": draw_query_broad(jax.random.fold_in(seeds[17], 71), 0),
        "latent": centred(seeds[3], (TOKENS, KV_RANK), 1.0, 6.0, ((0, 16),)),
        "rope_key": draw_rope_key(jax.random.fold_in(seeds[17], 71), 0),
        "latent_gain": jnp.clip(1.0 + 0.18 * jax.random.normal(seeds[5], (KV_RANK,), jnp.float32), 0.1, 1.9),
        "key_up_lean": centred(seeds[6], (KV_RANK, HEADS_A, NOPE_A), KV_RANK ** -0.5, 0.375, ((1, 2),)),
        "key_up_broad": centred(seeds[7], (KV_RANK, HEADS_B, NOPE_B), KV_RANK ** -0.5, 0.375, ((1, 2),)),
        "value_up_lean": centred(seeds[8], (KV_RANK, HEADS_A, V_A), KV_RANK ** -0.5, 0.375, ((1, 2),)),
        "value_up_broad": centred(seeds[9], (KV_RANK, HEADS_B, V_B), KV_RANK ** -0.5, 0.375, ((1, 2),)),
        "out_lean": centred(seeds[10], (HEADS_A, V_A, D), (HEADS_A * V_A + HEADS_B * V_B) ** -0.5, 0.15625, ((0, 2),)),
        "out_broad": centred(seeds[11], (HEADS_B, V_B, D), (HEADS_A * V_A + HEADS_B * V_B) ** -0.5, 0.15625, ((0, 2),)),
        "attn_gain": jnp.clip(1.0 + 0.18 * jax.random.normal(seeds[12], (D,), jnp.float32), 0.1, 1.9),
        "mlp_gain": jnp.clip(1.0 + 0.18 * jax.random.normal(seeds[13], (D,), jnp.float32), 0.1, 1.9),
        "gate_weight": centred(seeds[14], (D, FF), D ** -0.5, 0.125, ((0, 16), (1, 2))),
        "up_weight": centred(seeds[15], (D, FF), D ** -0.5, 0.125, ((0, 16), (1, 2))),
        "down_weight": centred(seeds[16], (FF, D), FF ** -0.5, 0.109375, ((0, 2), (1, 16))),
    }


THETA = 10000.0
EPS = 1e-06
NEGATIVE = -1e+30

def rotate(values, positions):
    width = values.shape[-1]
    half = width // 2
    freqs = THETA ** (-2.0 * jnp.arange(half, dtype=jnp.float32) / width)
    angle = positions.astype(jnp.float32)[:, None] * freqs[None, :]
    cosine = jnp.cos(angle)
    sine = jnp.sin(angle)
    if values.ndim == 3:
        cosine = cosine[:, None, :]
        sine = sine[:, None, :]
    first = values[..., :half]
    second = values[..., half:]
    return jnp.concatenate([first * cosine - second * sine, first * sine + second * cosine], axis=-1)

def normalize(values, gain):
    return values * lax.rsqrt(lax.optimization_barrier(jnp.mean(values * values, axis=-1, keepdims=True)) + EPS) * gain.astype(jnp.float32)

def widen(values):
    return lax.optimization_barrier(values).astype(jnp.float32)

def attend_group(query, key_up, value_up, latent_normed, rotated_key, positions):
    nope = key_up.shape[2]
    heads = key_up.shape[1]
    vsize = value_up.shape[2]
    scale = query.shape[2] ** (-0.5)
    lat = latent_normed.astype(jnp.float32)
    keys = widen(jnp.einsum('kr,rhd->khd', lat, key_up.astype(jnp.float32)).astype(jnp.bfloat16))
    values = widen(jnp.einsum('kr,rhd->khd', lat, value_up.astype(jnp.float32)).astype(jnp.bfloat16))
    rot_keys = rotated_key.astype(jnp.float32)
    query_nope = query[:, :, :nope].astype(jnp.float32)
    query_rot = widen(rotate(query[:, :, nope:].astype(jnp.float32), positions).astype(jnp.bfloat16))
    size = math.gcd(TOKENS, 256)

    def block(index):
        start = (index * size).astype(jnp.int32)
        rows = start + jnp.arange(size, dtype=jnp.int32)
        part_nope = lax.dynamic_slice_in_dim(query_nope, start, size, 0)
        part_rot = lax.dynamic_slice_in_dim(query_rot, start, size, 0)
        scores = (jnp.einsum('qhd,khd->hqk', part_nope, keys) + jnp.einsum('qhr,kr->hqk', part_rot, rot_keys)) * scale
        visible = positions[None, :] <= rows[:, None]
        scores = jnp.where(visible[None], scores, NEGATIVE)
        peak = lax.optimization_barrier(jnp.max(scores, axis=-1, keepdims=True))
        weights = jnp.where(visible[None], jnp.exp(scores - peak), 0.0)
        total = lax.optimization_barrier(jnp.sum(weights, axis=-1))
        rounded = widen(weights.astype(jnp.bfloat16))
        result = jnp.einsum('hqk,khv->qhv', rounded, values) / jnp.transpose(total)[:, :, None]
        return result.astype(jnp.bfloat16)
    blocks = lax.map(block, jnp.arange(TOKENS // size, dtype=jnp.int32))
    return blocks.reshape(TOKENS, heads, vsize)

def reference(residual_in, query_lean, query_broad, latent, rope_key, latent_gain, key_up_lean, key_up_broad, value_up_lean, value_up_broad, out_lean, out_broad, attn_gain, mlp_gain, gate_weight, up_weight, down_weight):
    positions = jnp.arange(TOKENS, dtype=jnp.int32)
    latent_normed = normalize(latent.astype(jnp.float32), latent_gain).astype(jnp.bfloat16)
    rotated_key = rotate(rope_key.astype(jnp.float32), positions).astype(jnp.bfloat16)
    attended_lean = attend_group(query_lean, key_up_lean, value_up_lean, latent_normed, rotated_key, positions)
    attended_broad = attend_group(query_broad, key_up_broad, value_up_broad, latent_normed, rotated_key, positions)
    lean_per = HEADS_A // N_TP
    broad_per = HEADS_B // N_TP
    head_sum = jnp.zeros((TOKENS, D), jnp.float32)
    for group in range(N_TP):
        partial_value = jnp.einsum('qhv,hvd->qd', attended_lean[:, group * lean_per:(group + 1) * lean_per].astype(jnp.float32), out_lean[group * lean_per:(group + 1) * lean_per].astype(jnp.float32))
        partial_value = partial_value + jnp.einsum('qhv,hvd->qd', attended_broad[:, group * broad_per:(group + 1) * broad_per].astype(jnp.float32), out_broad[group * broad_per:(group + 1) * broad_per].astype(jnp.float32))
        head_sum = head_sum + partial_value.astype(jnp.bfloat16).astype(jnp.float32)
    branch = normalize(head_sum, attn_gain)
    mixed = (residual_in.astype(jnp.float32) + branch).astype(jnp.bfloat16)
    normed = normalize(mixed.astype(jnp.float32), mlp_gain).astype(jnp.bfloat16)
    gate = jnp.dot(normed, gate_weight, preferred_element_type=jnp.float32)
    up = jnp.dot(normed, up_weight, preferred_element_type=jnp.float32)
    hidden = (jax.nn.silu(gate) * up).astype(jnp.bfloat16)
    units = FF // N_TP
    channel_sum = jnp.zeros((TOKENS, D), jnp.float32)
    for group in range(N_TP):
        partial_value = jnp.dot(hidden[:, group * units:(group + 1) * units], down_weight[group * units:(group + 1) * units], preferred_element_type=jnp.float32)
        channel_sum = channel_sum + partial_value.astype(jnp.bfloat16).astype(jnp.float32)
    return (mixed.astype(jnp.float32) + 0.5 * channel_sum).astype(jnp.bfloat16)
```

```python
import functools
import math

import jax
import jax.numpy as jnp
from jax import lax
from jax.experimental import pallas as pl
from jax.experimental.pallas import tpu as pltpu
from jax.sharding import PartitionSpec as P

THETA = 10000.0
EPS = 1e-06
NEGATIVE = -1e30


def rotate(values, positions):
    width = values.shape[-1]
    half = width // 2
    freqs = THETA ** (-2.0 * jnp.arange(half, dtype=jnp.float32) / width)
    angle = positions.astype(jnp.float32)[:, None] * freqs[None, :]
    cosine = jnp.cos(angle)
    sine = jnp.sin(angle)
    if values.ndim == 3:
        cosine = cosine[:, None, :]
        sine = sine[:, None, :]
    first = values[..., :half]
    second = values[..., half:]
    return jnp.concatenate(
        [first * cosine - second * sine, first * sine + second * cosine], axis=-1
    )


def normalize(values, gain):
    return values * lax.rsqrt(jnp.mean(values * values, axis=-1, keepdims=True) + EPS) * gain


def block_keys(weights, latent_rows):
    projected = []
    for key_up, value_up in weights:
        keys = jnp.einsum(
            "kr,rhd->khd", latent_rows, key_up, preferred_element_type=jnp.float32
        ).astype(jnp.bfloat16)
        values = jnp.einsum(
            "kr,rhd->khd", latent_rows, value_up, preferred_element_type=jnp.float32
        ).astype(jnp.bfloat16)
        projected.append((keys, values))
    return projected


def attend(carry, queries, projected, rotated_rows, key_pos, query_pos):
    updated = []
    visible = key_pos[None, :] <= query_pos[:, None]
    for state, query, pair in zip(carry, queries, projected):
        query_nope, query_rot, scale = query
        keys, values = pair
        peak, total, accum = state
        scores = (
            jnp.einsum("qhd,khd->hqk", query_nope, keys, preferred_element_type=jnp.float32)
            + jnp.einsum("qhr,kr->hqk", query_rot, rotated_rows, preferred_element_type=jnp.float32)
        ) * scale
        scores = jnp.where(visible[None], scores, NEGATIVE)
        new_peak = jnp.maximum(peak, jnp.max(scores, axis=-1))
        weights = jnp.where(visible[None], jnp.exp(scores - new_peak[..., None]), 0.0)
        factor = jnp.exp(peak - new_peak)
        total = total * factor + jnp.sum(weights, axis=-1)
        accum = accum * factor[..., None] + jnp.einsum(
            "hqk,khv->hqv", weights.astype(jnp.bfloat16), values, preferred_element_type=jnp.float32
        )
        updated.append((new_peak, total, accum))
    return tuple(updated)


def fold_piece(carry, latent_piece, rotated_piece, piece_pos, weights, segments):
    count = latent_piece.shape[0]
    block = math.gcd(count, 1024)
    last_all = segments[0][1][-1]

    def one_block(index, state):
        lat_rows = lax.dynamic_slice_in_dim(latent_piece, index * block, block, 0)
        rot_rows = lax.dynamic_slice_in_dim(rotated_piece, index * block, block, 0)
        pos_rows = lax.dynamic_slice_in_dim(piece_pos, index * block, block, 0)
        first_key = jnp.min(pos_rows)

        def work(inner):
            projected = block_keys(weights, lat_rows)
            results = []
            for inner_seg, segment in zip(inner, segments):
                queries, seg_pos = segment
                results.append(
                    lax.cond(
                        first_key <= seg_pos[-1],
                        lambda held, queries=queries, seg_pos=seg_pos: attend(
                            held, queries, projected, rot_rows, pos_rows, seg_pos
                        ),
                        lambda held: held,
                        inner_seg,
                    )
                )
            return tuple(results)

        return lax.cond(first_key <= last_all, work, lambda inner: inner, state)

    return lax.fori_loop(0, count // block, one_block, carry)


def shards(
    residual_in,
    query_lean,
    query_broad,
    latent,
    rope_key,
    latent_gain,
    key_up_lean,
    key_up_broad,
    value_up_lean,
    value_up_broad,
    out_lean,
    out_broad,
    attn_gain,
    mlp_gain,
    gate_weight,
    up_weight,
    down_weight,
):
    tokens_here = query_lean.shape[0]
    n_tp = lax.axis_size("tp")
    share = tokens_here // n_tp
    sp_index = lax.axis_index("sp")
    first = sp_index * tokens_here
    query_pos = first + jnp.arange(tokens_here, dtype=jnp.int32)
    rope_width = rope_key.shape[1]
    weights = ((key_up_lean, value_up_lean), (key_up_broad, value_up_broad))
    segment_rows = (query_lean, query_broad, query_pos)
    segments = []
    initial = []
    lean_rows, broad_rows, seg_pos = segment_rows
    queries = []
    states = []
    for query, value_up in ((lean_rows, value_up_lean), (broad_rows, value_up_broad)):
        nope = query.shape[2] - rope_width
        query_rot = rotate(query[:, :, nope:].astype(jnp.float32), seg_pos).astype(jnp.bfloat16)
        queries.append((query[:, :, :nope], query_rot, query.shape[2] ** (-0.5)))
        heads = query.shape[1]
        rows = query.shape[0]
        states.append(
            (
                jnp.full((heads, rows), NEGATIVE, jnp.float32),
                jnp.zeros((heads, rows), jnp.float32),
                jnp.zeros((heads, rows, value_up.shape[2]), jnp.float32),
            )
        )
    segments.append((tuple(queries), seg_pos))
    initial.append(tuple(states))
    segments = tuple(segments)
    initial = tuple(initial)
    sent_latent = normalize(latent.astype(jnp.float32), latent_gain).astype(jnp.bfloat16)
    sent_rot = rotate(rope_key.astype(jnp.float32), query_pos).astype(jnp.bfloat16)
    pieces = (
        lax.all_gather(sent_latent, "sp", axis=0, tiled=True),
        lax.all_gather(sent_rot, "sp", axis=0, tiled=True),
    )
    piece_pos = jnp.arange(pieces[0].shape[0], dtype=jnp.int32)
    folded = fold_piece(initial, pieces[0], pieces[1], piece_pos, weights, segments)
    results = [
        [(accum / total[..., None]).astype(jnp.bfloat16) for peak, total, accum in seg_state]
        for seg_state in folded
    ]
    attended = results[0]
    term = jnp.zeros((share * lax.axis_size("tp"), out_lean.shape[2]), jnp.float32)
    for rows_all, weight in ((attended[0], out_lean), (attended[1], out_broad)):
        rows = rows_all
        term = term + jnp.einsum("hqv,hvd->qd", rows, weight, preferred_element_type=jnp.float32)
    head_sum = lax.psum_scatter(
        term.astype(jnp.bfloat16), "tp", scatter_dimension=0, tiled=True
    ).astype(jnp.float32)
    branch = normalize(head_sum, attn_gain)
    kept = (residual_in.astype(jnp.float32) + branch).astype(jnp.bfloat16)
    normed = normalize(kept.astype(jnp.float32), mlp_gain).astype(jnp.bfloat16)
    whole_normed = lax.all_gather(normed, "tp", axis=0, tiled=True)
    gate_whole, up_whole, down_whole = (
        lax.all_gather(gate_weight, "sp", axis=0, tiled=True),
        lax.all_gather(up_weight, "sp", axis=0, tiled=True),
        lax.all_gather(down_weight, "sp", axis=1, tiled=True),
    )
    gate = jnp.dot(whole_normed, gate_whole, preferred_element_type=jnp.float32)
    up = jnp.dot(whole_normed, up_whole, preferred_element_type=jnp.float32)
    hidden = (jax.nn.silu(gate) * up).astype(jnp.bfloat16)
    rows = hidden
    channel_sum = lax.psum_scatter(
        jnp.dot(rows, down_whole, preferred_element_type=jnp.float32).astype(jnp.bfloat16),
        "tp",
        scatter_dimension=0,
        tiled=True,
    ).astype(jnp.float32)
    return (kept.astype(jnp.float32) + 0.5 * channel_sum).astype(jnp.bfloat16)


LOG2E = math.log2(math.e)


def grid_of(mesh):
    n_sp, n_tp = mesh.shape["sp"], mesh.shape["tp"]
    devices = mesh.devices.reshape(n_sp, n_tp)
    try:
        places = [tuple(device.coords) for device in devices[:, 0]]
        partners = [tuple(device.coords) for device in devices[:, -1]]
    except Exception:
        return (n_sp // 4, 2, 2) if n_sp % 4 == 0 else None
    if places != partners:
        return None
    low = [min(place[k] for place in places) for k in range(3)]
    sizes = [max(place[k] for place in places) - low[k] + 1 for k in range(3)]
    wide_z, wide_y, wide_x = sizes[2], sizes[1], sizes[0]
    if wide_z * wide_y * wide_x != n_sp:
        return None
    for index, place in enumerate(places):
        x, y, z = (place[k] - low[k] for k in range(3))
        if (z * wide_y + y) * wide_x + x != index:
            return None
    return wide_z, wide_y, wide_x


def hop_table(grid):
    wide_z = grid[0]
    entries = [
        (dz, fy, fx)
        for dz in range(1 - wide_z, wide_z)
        for fy in range(2)
        for fx in range(2)
        if (dz, fy, fx) != (0, 0, 0)
    ]
    entries.sort(key=lambda e: (abs(e[0]) + e[1] + e[2], abs(e[0]), e))
    return entries


def layer_kernel(
    grid, shapes, res, ql, qb, lat, lrow, ag, mg, kul, kub, vu, wol, wob, gw, uw, dw, out,
    lat_all, gate_all, up_all, down_all, ktl, ktb, vals, peak, total, acc, att, term, inbox, kept,
    normed, hidden, inbox2, lat_recv, lat_send, lat_pair, recv, send, own_sem, pair_send, pair_recv,
):
    wide_z, wide_y, wide_x = grid
    n_sp = wide_z * wide_y * wide_x
    tokens, share, rope = shapes
    heads_l, heads_b = ql.shape[0], qb.shape[0]
    bf16, f32 = jnp.bfloat16, jnp.float32
    me = lax.axis_index("sp")
    core = lax.axis_index("tp")
    my_x = lax.rem(me, wide_x)
    my_y = lax.rem(me // wide_x, wide_y)
    my_z = me // (wide_x * wide_y)
    here = (my_z, my_y, my_x)
    strides = (wide_y * wide_x, wide_x, 1)
    Z, Y, X = 0, 1, 2
    flip_y = me + (1 - 2 * my_y) * strides[1]
    flip_x = me + (1 - 2 * my_x)
    ways = (
        (X, None, None, flip_x),
        (Y, None, None, flip_y),
        (Z, -1, my_z > 0, jnp.maximum(me - strides[0], 0)),
        (Z, 1, my_z < wide_z - 1, jnp.minimum(me + strides[0], n_sp - 1)),
    )

    barrier = pltpu.get_barrier_semaphore()
    for dim, sign, exists, where in ways:
        def greet(where=where):
            pl.semaphore_signal(barrier, inc=1, device_id={"sp": where})
        if exists is None:
            greet()
        else:
            pl.when(exists)(greet)
    pl.semaphore_signal(barrier, inc=1, device_id={"tp": 1 - core})
    ends = jnp.where(my_z > 0, 1, 0) + jnp.where(my_z < wide_z - 1, 1, 0)
    pl.semaphore_wait(barrier, 3 + ends)

    def wanted(order, origin, way):
        dim, sign, exists, _ = way
        place = order.index(dim)
        ok = origin[dim] == here[dim] if sign is None else sign * (here[dim] - origin[dim]) >= 0
        for later in order[place + 1:]:
            ok = jnp.logical_and(ok, origin[later] == here[later])
        return ok if exists is None else jnp.logical_and(ok, exists)

    def index_of(origin):
        return origin[0] * strides[0] + origin[1] * strides[1] + origin[2]

    gate_rows, units = gw.shape
    down_cols = dw.shape[1]
    cut = units // 4
    ORDER_A, ORDER_B, ORDER_C, ORDER_D = (Z, X, Y), (Z, Y, X), (X, Y, Z), (Y, X, Z)

    def gate_at(ref):
        return lambda i: ref.at[pl.ds(pl.multiple_of(i * gate_rows, gate_rows), gate_rows)]

    def down_at(k):
        return lambda i: down_all.at[
            pl.ds(k * cut, cut), pl.ds(pl.multiple_of(i * down_cols, down_cols), down_cols)
        ]

    parts = [
        (ORDER_A, gw, gate_at(gate_all)),
        (ORDER_B, uw, gate_at(up_all)),
    ] + [
        (order, dw.at[pl.ds(k * cut, cut)], down_at(k))
        for k, order in enumerate((ORDER_A, ORDER_B, ORDER_C, ORDER_D))
    ]

    def part_copy(p, w, i, mine):
        order, own, at = parts[p]
        return pltpu.make_async_remote_copy(
            src_ref=own if mine else at(i), dst_ref=at(i), send_sem=send.at[p, w, i],
            recv_sem=recv.at[p, i], device_id={"sp": ways[w][3]},
        )

    half = lat.shape[0] // 2
    first = pl.multiple_of(core * half, half)

    def lat_at(i):
        return lat_all.at[i, pl.ds(first, half)]

    def lat_copy(w, i, mine):
        return pltpu.make_async_remote_copy(
            src_ref=lat.at[pl.ds(first, half)] if mine else lat_at(i), dst_ref=lat_at(i),
            send_sem=lat_send.at[w, i], recv_sem=lat_recv.at[i], device_id={"sp": ways[w][3]},
        )

    def pair_lat(i):
        return pltpu.make_async_remote_copy(
            src_ref=lat_at(i), dst_ref=lat_at(i), send_sem=lat_pair.at[0, i],
            recv_sem=lat_pair.at[1, i], device_id={"tp": 1 - core},
        )

    def run(condition, action):
        if condition is None:
            action()
        else:
            pl.when(condition)(action)

    for w, way in enumerate(ways):
        run(way[2], lambda w=w: lat_copy(w, me, True).start())
    own = [pltpu.make_async_copy(lat, lat_all.at[me], own_sem.at[0])]
    for p, (_, src, at) in enumerate(parts):
        own.append(pltpu.make_async_copy(src, at(me), own_sem.at[1 + p]))
    for copy in own:
        copy.start()

    def send_own(w):
        for p in range(len(parts)):
            run(ways[w][2], lambda p=p: part_copy(p, w, me, True).start())

    send_own(0)

    table = hop_table(grid)
    codes = [((dz + wide_z - 1) * 2 + fy) * 2 + fx for dz, fy, fx in table]
    per = 4
    words = [
        sum(code << (7 * k) for k, code in enumerate(codes[at:at + per]))
        for at in range(0, len(codes), per)
    ]

    def origin_of(n):
        word = jnp.int32(words[0])
        for k in range(1, len(words)):
            word = jnp.where(n // per == k, jnp.int32(words[k]), word)
        rem = lax.rem(n, per)
        for k in range(1, per):
            word = jnp.where(rem >= k, word // 128, word)
        code = lax.rem(word, 128)
        dz = code // 4 - (wide_z - 1)
        fy = lax.rem(code // 2, 2)
        fx = lax.rem(code, 2)
        oz = my_z + dz
        oy = my_y + fy * (1 - 2 * my_y)
        ox = my_x + fx * (1 - 2 * my_x)
        return (oz, oy, ox), jnp.logical_and(oz >= 0, oz < wide_z)

    def lat_event(n, _):
        origin, valid = origin_of(n)

        @pl.when(valid)
        def _():
            i = index_of(origin)
            lat_copy(0, i, False).wait_recv()
            for w, way in enumerate(ways):
                run(wanted(ORDER_C, origin, way), lambda w=w: lat_copy(w, i, False).start())
            pair_lat(i).start()

        return 0

    def part_event(n, _):
        origin, valid = origin_of(n)

        @pl.when(valid)
        def _():
            i = index_of(origin)
            for p, (order, _, _) in enumerate(parts):
                part_copy(p, 0, i, False).wait_recv()
                for w, way in enumerate(ways):
                    run(wanted(order, origin, way), lambda p=p, w=w: part_copy(p, w, i, False).start())

        return 0

    count = len(table)
    early = sum(1 for dz, fy, fx in table if abs(dz) + fy + fx <= 2)
    lax.fori_loop(0, early, lat_event, 0)
    send_own(1)
    lax.fori_loop(early, count, lat_event, 0)
    send_own(2)
    send_own(3)
    for copy in own:
        copy.wait()

    def lat_arrived(i, _):
        pl.when(i != me)(lambda: pair_lat(i).wait_recv())
        return 0

    lax.fori_loop(0, n_sp, lat_arrived, 0)

    peak[...] = jnp.full(peak.shape, NEGATIVE, f32)
    total[...] = jnp.zeros(total.shape, f32)
    acc[...] = jnp.zeros(acc.shape, f32)
    wide_l = kul.shape[0] // heads_l
    wide_b = kub.shape[0] // heads_b
    lanes = 2 * wide_l
    contract = (((1,), (1,)), ((), ()))

    def attend_block(j):
        rows = lat_all[j, :tokens, :]
        rot = lat_all[j, tokens:, :]
        for ups, keys, heads, wide in ((kul, ktl, heads_l, wide_l), (kub, ktb, heads_b, wide_b)):
            made = lax.dot_general(ups[...], rows, contract, preferred_element_type=f32).astype(bf16)
            for h in range(heads):
                keys[h, :wide, :] = made[h * wide:(h + 1) * wide]
                keys[h, wide:, :] = rot
        vals[...] = jnp.dot(rows, vu[...], preferred_element_type=f32).astype(bf16)
        row_pos = lax.broadcasted_iota(jnp.int32, (tokens, tokens), 0) + (me - j) * tokens
        visible = lax.broadcasted_iota(jnp.int32, (tokens, tokens), 1) <= row_pos
        for g in range(heads_l + heads_b):
            if g < heads_l:
                query, keys, col = ql[g], ktl[g], (g // 2) * lanes
            else:
                query, keys = qb[g - heads_l], ktb[g - heads_l]
                col = heads_l * wide_l + (g - heads_l) * wide_b
            scores = jnp.dot(query, keys, preferred_element_type=f32) * (
                LOG2E * query.shape[1] ** (-0.5)
            )
            scores = jnp.where(visible, scores, NEGATIVE)
            old = peak[g]
            new = jnp.maximum(old, jnp.max(scores, axis=-1, keepdims=True))
            weights = jnp.exp2(scores - new)
            factor = jnp.exp2(old - new)
            peak[g] = new
            total[g] = total[g] * factor + jnp.sum(weights, axis=-1, keepdims=True)
            acc[g] = acc[g] * factor + jnp.dot(
                weights.astype(bf16), vals[:, col:col + wide_b], preferred_element_type=f32
            )

    def step(j, _):
        lax.fori_loop((j * early) // n_sp, ((j + 1) * early) // n_sp, part_event, 0)
        pl.when(j <= me)(lambda: attend_block(j))
        return 0

    lax.fori_loop(0, n_sp, step, 0)

    low = lax.broadcasted_iota(jnp.int32, (tokens, lanes), 1) < wide_l
    for pair in range(heads_l // 2):
        both = [acc[2 * pair + k] / total[2 * pair + k] for k in range(2)]
        att[:, pair * lanes:(pair + 1) * lanes] = jnp.where(low, both[0], both[1]).astype(bf16)
    split = heads_l * wide_l
    for h in range(heads_b):
        g = heads_l + h
        att[:, split + h * wide_b:split + (h + 1) * wide_b] = (acc[g] / total[g]).astype(bf16)

    features = out.shape[1]
    block = math.gcd(features, 512)

    def project(n, _):
        cols = pl.ds(pl.multiple_of(n * block, block), block)
        term[:, cols] = (
            jnp.dot(att[:, :split], wol[:, cols], preferred_element_type=f32)
            + jnp.dot(att[:, split:], wob[:, cols], preferred_element_type=f32)
        ).astype(bf16)
        return 0

    lax.fori_loop(0, features // block, project, 0)
    mine = pl.ds(pl.multiple_of(core * share, share), share)
    theirs = pl.ds(pl.multiple_of((1 - core) * share, share), share)

    def to_pair(k, src, dst):
        return pltpu.make_async_remote_copy(
            src_ref=src, dst_ref=dst, send_sem=pair_send.at[k], recv_sem=pair_recv.at[k],
            device_id={"tp": 1 - core},
        )

    heads_out = to_pair(0, term.at[theirs], inbox)
    heads_out.start()
    heads_out.wait_recv()
    rows_at_once = math.gcd(share, 16)

    def norms(n, _):
        rows = pl.ds(pl.multiple_of(n * rows_at_once, rows_at_once), rows_at_once)
        full = pl.ds(pl.multiple_of(core * share + n * rows_at_once, rows_at_once), rows_at_once)
        summed = term[full, :].astype(f32) + inbox[rows, :].astype(f32)
        branch = normalize(summed, ag[...])
        mixed = (res[rows, :].astype(f32) + branch).astype(bf16)
        kept[rows, :] = mixed
        normed[full, :] = normalize(mixed.astype(f32), mg[...]).astype(bf16)
        return 0

    lax.fori_loop(0, share // rows_at_once, norms, 0)
    rows_out = to_pair(1, normed.at[mine], normed.at[mine])
    rows_out.start()
    lax.fori_loop(early, count, part_event, 0)
    to_pair(1, normed.at[theirs], normed.at[theirs]).wait_recv()

    def feed(cols):
        gate = jnp.dot(normed[...], gate_all[:, cols], preferred_element_type=f32)
        up = jnp.dot(normed[...], up_all[:, cols], preferred_element_type=f32)
        hidden[:, cols] = (gate / (1.0 + jnp.exp(-gate)) * up).astype(bf16)

    span = 256

    def feed_loop(n, _):
        feed(pl.ds(pl.multiple_of(n * span, span), span))
        return 0

    lax.fori_loop(0, units // span, feed_loop, 0)
    if units % span:
        feed(pl.ds(units // span * span, units % span))
    heads_out.wait_send()
    wide_n = math.gcd(features, 256)

    def down(n, _):
        cols = pl.ds(pl.multiple_of(n * wide_n, wide_n), wide_n)
        term[:, cols] = jnp.dot(
            hidden[...], down_all[:, cols], preferred_element_type=f32
        ).astype(bf16)
        return 0

    lax.fori_loop(0, features // wide_n, down, 0)
    sums_out = to_pair(2, term.at[theirs], inbox2)
    sums_out.start()

    def sent(i, _):
        origin = (i // strides[0], lax.rem(i // strides[1], wide_y), lax.rem(i, wide_x))
        for w, way in enumerate(ways):
            run(wanted(ORDER_C, origin, way), lambda w=w: lat_copy(w, i, False).wait_send())
            for p, (order, _, _) in enumerate(parts):
                run(wanted(order, origin, way), lambda p=p, w=w: part_copy(p, w, i, False).wait_send())
        pl.when(i != me)(lambda: pair_lat(i).wait_send())
        return 0

    lax.fori_loop(0, n_sp, sent, 0)
    rows_out.wait_send()
    sums_out.wait_recv()

    def finish(n, _):
        rows = pl.ds(pl.multiple_of(n * rows_at_once, rows_at_once), rows_at_once)
        full = pl.ds(pl.multiple_of(core * share + n * rows_at_once, rows_at_once), rows_at_once)
        summed = term[full, :].astype(f32) + inbox2[rows, :].astype(f32)
        out[rows, :] = (kept[rows, :].astype(f32) + 0.5 * summed).astype(bf16)
        return 0

    lax.fori_loop(0, share // rows_at_once, finish, 0)
    sums_out.wait_send()


def fused_shards(
    grid, residual_in, query_lean, query_broad, latent, rope_key, latent_gain, key_up_lean,
    key_up_broad, value_up_lean, value_up_broad, out_lean, out_broad, attn_gain, mlp_gain,
    gate_weight, up_weight, down_weight,
):
    bf16, f32 = jnp.bfloat16, jnp.float32
    tokens = query_lean.shape[0]
    share, features = residual_in.shape
    rank = latent.shape[1]
    rope = rope_key.shape[1]
    n_sp = lax.axis_size("sp")
    positions = lax.axis_index("sp") * tokens + jnp.arange(tokens, dtype=jnp.int32)

    def turned(query):
        nope = query.shape[2] - rope
        rot = rotate(query[:, :, nope:].astype(f32), positions).astype(bf16)
        return jnp.transpose(jnp.concatenate([query[:, :, :nope], rot], axis=-1), (1, 0, 2))

    ql, qb = turned(query_lean), turned(query_broad)
    lat = normalize(latent.astype(f32), latent_gain).astype(bf16)
    rot_key = rotate(rope_key.astype(f32), positions).astype(bf16)
    lat = jnp.concatenate([lat, rot_key.T], axis=0)
    kul = key_up_lean.reshape(rank, -1).T
    kub = key_up_broad.reshape(rank, -1).T
    vu = jnp.concatenate([value_up_lean.reshape(rank, -1), value_up_broad.reshape(rank, -1)], axis=1)
    wol = out_lean.reshape(-1, features)
    wob = out_broad.reshape(-1, features)
    heads = ql.shape[0] + qb.shape[0]
    units = gate_weight.shape[1]
    wide_b = value_up_broad.shape[2]
    vmem = pl.BlockSpec(memory_space=pltpu.VMEM)
    args = (
        residual_in, ql, qb, lat, lat[:1], attn_gain[None], mlp_gain[None], kul, kub, vu, wol, wob,
        gate_weight, up_weight, down_weight,
    )
    dma = pltpu.SemaphoreType.DMA
    return pl.pallas_call(
        functools.partial(layer_kernel, grid, (tokens, share, rope)),
        out_shape=jax.ShapeDtypeStruct((share, features), bf16),
        in_specs=[vmem] * len(args),
        out_specs=vmem,
        scratch_shapes=[
            pltpu.VMEM((n_sp, tokens + rope, rank), bf16),
            pltpu.VMEM((features, units), bf16),
            pltpu.VMEM((features, units), bf16),
            pltpu.VMEM((units, features), bf16),
            pltpu.VMEM((ql.shape[0], ql.shape[2], tokens), bf16),
            pltpu.VMEM((qb.shape[0], qb.shape[2], tokens), bf16),
            pltpu.VMEM((tokens, vu.shape[1]), bf16),
            pltpu.VMEM((heads, tokens, 1), f32),
            pltpu.VMEM((heads, tokens, 1), f32),
            pltpu.VMEM((heads, tokens, wide_b), f32),
            pltpu.VMEM((tokens, vu.shape[1]), bf16),
            pltpu.VMEM((tokens, features), bf16),
            pltpu.VMEM((share, features), bf16),
            pltpu.VMEM((share, features), bf16),
            pltpu.VMEM((tokens, features), bf16),
            pltpu.VMEM((tokens, units), bf16),
            pltpu.VMEM((share, features), bf16),
            dma((n_sp,)),
            dma((4, n_sp)),
            dma((2, n_sp)),
            dma((6, n_sp)),
            dma((6, 4, n_sp)),
            dma((7,)),
            dma((3,)),
            dma((3,)),
        ],
        compiler_params=pltpu.CompilerParams(
            collective_id=0, has_side_effects=True, vmem_limit_bytes=62 * 2**20
        ),
    )(*args)


def fits(grid, mesh, args):
    if grid is None or mesh.shape["tp"] != 2 or grid[1] != 2 or grid[2] != 2 or grid[0] > 8:
        return False
    n_sp = mesh.shape["sp"]
    tokens = args[1].shape[0] // n_sp
    share = tokens // 2
    units = args[14].shape[1] // 2
    heads_l, heads_b = args[6].shape[1] // 2, args[7].shape[1] // 2
    wide_l, wide_b = args[6].shape[2], args[7].shape[2]
    rope = args[4].shape[1]
    return (
        tokens % 128 == 0 and tokens <= 256 and share % 16 == 0 and units % 128 == 0
        and units % 64 == 0 and heads_l % 2 == 0 and 2 * wide_l == wide_b and wide_b % 128 == 0
        and args[3].shape[1] == tokens and rope % 16 == 0 and (tokens + rope) % 32 == 0
        and heads_b > 0 and args[8].shape[2] == wide_l and args[9].shape[2] == wide_b
        and (args[14].shape[0] // n_sp) % 16 == 0 and (args[16].shape[1] // n_sp) % 128 == 0
    )


def solution(mesh):
    in_specs = (
        P(("sp", "tp"), None),
        P("sp", "tp", None),
        P("sp", "tp", None),
        P("sp", None),
        P("sp", None),
        P(),
        P(None, "tp", None),
        P(None, "tp", None),
        P(None, "tp", None),
        P(None, "tp", None),
        P("tp", None, None),
        P("tp", None, None),
        P(),
        P(),
        P("sp", "tp"),
        P("sp", "tp"),
        P("tp", "sp"),
    )
    out_specs = P(("sp", "tp"), None)
    grid = grid_of(mesh)

    def layer(*args):
        body = functools.partial(fused_shards, grid) if fits(grid, mesh, args) else shards
        return jax.shard_map(
            body, mesh=mesh, in_specs=in_specs, out_specs=out_specs, check_vma=False
        )(*args)

    return layer
```

```python
import functools
import math

import jax
import jax.numpy as jnp
from jax import lax
from jax.experimental import pallas as pl
from jax.experimental.pallas import tpu as pltpu
from jax.sharding import PartitionSpec as P

THETA = 10000.0
EPS = 1e-06
NEGATIVE = -1e30


def rotate(values, positions):
    width = values.shape[-1]
    half = width // 2
    freqs = THETA ** (-2.0 * jnp.arange(half, dtype=jnp.float32) / width)
    angle = positions.astype(jnp.float32)[:, None] * freqs[None, :]
    cosine = jnp.cos(angle)
    sine = jnp.sin(angle)
    if values.ndim == 3:
        cosine = cosine[:, None, :]
        sine = sine[:, None, :]
    first = values[..., :half]
    second = values[..., half:]
    return jnp.concatenate(
        [first * cosine - second * sine, first * sine + second * cosine], axis=-1
    )


def normalize(values, gain):
    return values * lax.rsqrt(jnp.mean(values * values, axis=-1, keepdims=True) + EPS) * gain


def block_keys(weights, latent_rows):
    projected = []
    for key_up, value_up in weights:
        keys = jnp.einsum(
            "kr,rhd->khd", latent_rows, key_up, preferred_element_type=jnp.float32
        ).astype(jnp.bfloat16)
        values = jnp.einsum(
            "kr,rhd->khd", latent_rows, value_up, preferred_element_type=jnp.float32
        ).astype(jnp.bfloat16)
        projected.append((keys, values))
    return projected


def attend(carry, queries, projected, rotated_rows, key_pos, query_pos):
    updated = []
    visible = key_pos[None, :] <= query_pos[:, None]
    for state, query, pair in zip(carry, queries, projected):
        query_nope, query_rot, scale = query
        keys, values = pair
        peak, total, accum = state
        scores = (
            jnp.einsum("qhd,khd->hqk", query_nope, keys, preferred_element_type=jnp.float32)
            + jnp.einsum("qhr,kr->hqk", query_rot, rotated_rows, preferred_element_type=jnp.float32)
        ) * scale
        scores = jnp.where(visible[None], scores, NEGATIVE)
        new_peak = jnp.maximum(peak, jnp.max(scores, axis=-1))
        weights = jnp.where(visible[None], jnp.exp(scores - new_peak[..., None]), 0.0)
        factor = jnp.exp(peak - new_peak)
        total = total * factor + jnp.sum(weights, axis=-1)
        accum = accum * factor[..., None] + jnp.einsum(
            "hqk,khv->hqv", weights.astype(jnp.bfloat16), values, preferred_element_type=jnp.float32
        )
        updated.append((new_peak, total, accum))
    return tuple(updated)


def fold_piece(carry, latent_piece, rotated_piece, piece_pos, weights, segments):
    count = latent_piece.shape[0]
    block = math.gcd(count, 1024)
    last_all = segments[0][1][-1]

    def one_block(index, state):
        lat_rows = lax.dynamic_slice_in_dim(latent_piece, index * block, block, 0)
        rot_rows = lax.dynamic_slice_in_dim(rotated_piece, index * block, block, 0)
        pos_rows = lax.dynamic_slice_in_dim(piece_pos, index * block, block, 0)
        first_key = jnp.min(pos_rows)

        def work(inner):
            projected = block_keys(weights, lat_rows)
            results = []
            for inner_seg, segment in zip(inner, segments):
                queries, seg_pos = segment
                results.append(
                    lax.cond(
                        first_key <= seg_pos[-1],
                        lambda held, queries=queries, seg_pos=seg_pos: attend(
                            held, queries, projected, rot_rows, pos_rows, seg_pos
                        ),
                        lambda held: held,
                        inner_seg,
                    )
                )
            return tuple(results)

        return lax.cond(first_key <= last_all, work, lambda inner: inner, state)

    return lax.fori_loop(0, count // block, one_block, carry)


def shards(
    residual_in,
    query_lean,
    query_broad,
    latent,
    rope_key,
    latent_gain,
    key_up_lean,
    key_up_broad,
    value_up_lean,
    value_up_broad,
    out_lean,
    out_broad,
    attn_gain,
    mlp_gain,
    gate_weight,
    up_weight,
    down_weight,
):
    tokens_here = query_lean.shape[0]
    n_tp = lax.axis_size("tp")
    share = tokens_here // n_tp
    sp_index = lax.axis_index("sp")
    first = sp_index * tokens_here
    query_pos = first + jnp.arange(tokens_here, dtype=jnp.int32)
    rope_width = rope_key.shape[1]
    weights = ((key_up_lean, value_up_lean), (key_up_broad, value_up_broad))
    segment_rows = (query_lean, query_broad, query_pos)
    segments = []
    initial = []
    lean_rows, broad_rows, seg_pos = segment_rows
    queries = []
    states = []
    for query, value_up in ((lean_rows, value_up_lean), (broad_rows, value_up_broad)):
        nope = query.shape[2] - rope_width
        query_rot = rotate(query[:, :, nope:].astype(jnp.float32), seg_pos).astype(jnp.bfloat16)
        queries.append((query[:, :, :nope], query_rot, query.shape[2] ** (-0.5)))
        heads = query.shape[1]
        rows = query.shape[0]
        states.append(
            (
                jnp.full((heads, rows), NEGATIVE, jnp.float32),
                jnp.zeros((heads, rows), jnp.float32),
                jnp.zeros((heads, rows, value_up.shape[2]), jnp.float32),
            )
        )
    segments.append((tuple(queries), seg_pos))
    initial.append(tuple(states))
    segments = tuple(segments)
    initial = tuple(initial)
    sent_latent = normalize(latent.astype(jnp.float32), latent_gain).astype(jnp.bfloat16)
    sent_rot = rotate(rope_key.astype(jnp.float32), query_pos).astype(jnp.bfloat16)
    pieces = (
        lax.all_gather(sent_latent, "sp", axis=0, tiled=True),
        lax.all_gather(sent_rot, "sp", axis=0, tiled=True),
    )
    piece_pos = jnp.arange(pieces[0].shape[0], dtype=jnp.int32)
    folded = fold_piece(initial, pieces[0], pieces[1], piece_pos, weights, segments)
    results = [
        [(accum / total[..., None]).astype(jnp.bfloat16) for peak, total, accum in seg_state]
        for seg_state in folded
    ]
    attended = results[0]
    term = jnp.zeros((share * lax.axis_size("tp"), out_lean.shape[2]), jnp.float32)
    for rows_all, weight in ((attended[0], out_lean), (attended[1], out_broad)):
        rows = rows_all
        term = term + jnp.einsum("hqv,hvd->qd", rows, weight, preferred_element_type=jnp.float32)
    head_sum = lax.psum_scatter(
        term.astype(jnp.bfloat16), "tp", scatter_dimension=0, tiled=True
    ).astype(jnp.float32)
    branch = normalize(head_sum, attn_gain)
    kept = (residual_in.astype(jnp.float32) + branch).astype(jnp.bfloat16)
    normed = normalize(kept.astype(jnp.float32), mlp_gain).astype(jnp.bfloat16)
    whole_normed = lax.all_gather(normed, "tp", axis=0, tiled=True)
    gate_whole, up_whole, down_whole = (
        lax.all_gather(gate_weight, "sp", axis=0, tiled=True),
        lax.all_gather(up_weight, "sp", axis=0, tiled=True),
        lax.all_gather(down_weight, "sp", axis=1, tiled=True),
    )
    gate = jnp.dot(whole_normed, gate_whole, preferred_element_type=jnp.float32)
    up = jnp.dot(whole_normed, up_whole, preferred_element_type=jnp.float32)
    hidden = (jax.nn.silu(gate) * up).astype(jnp.bfloat16)
    rows = hidden
    channel_sum = lax.psum_scatter(
        jnp.dot(rows, down_whole, preferred_element_type=jnp.float32).astype(jnp.bfloat16),
        "tp",
        scatter_dimension=0,
        tiled=True,
    ).astype(jnp.float32)
    return (kept.astype(jnp.float32) + 0.5 * channel_sum).astype(jnp.bfloat16)


LOG2E = math.log2(math.e)


def grid_of(mesh):
    n_sp, n_tp = mesh.shape["sp"], mesh.shape["tp"]
    devices = mesh.devices.reshape(n_sp, n_tp)
    try:
        places = [tuple(device.coords) for device in devices[:, 0]]
        partners = [tuple(device.coords) for device in devices[:, -1]]
    except Exception:
        return (n_sp // 4, 2, 2) if n_sp % 4 == 0 else None
    if places != partners:
        return None
    low = [min(place[k] for place in places) for k in range(3)]
    sizes = [max(place[k] for place in places) - low[k] + 1 for k in range(3)]
    wide_z, wide_y, wide_x = sizes[2], sizes[1], sizes[0]
    if wide_z * wide_y * wide_x != n_sp:
        return None
    for index, place in enumerate(places):
        x, y, z = (place[k] - low[k] for k in range(3))
        if (z * wide_y + y) * wide_x + x != index:
            return None
    return wide_z, wide_y, wide_x


def hop_table(grid):
    wide_z = grid[0]
    entries = [
        (dz, fy, fx)
        for dz in range(1 - wide_z, wide_z)
        for fy in range(2)
        for fx in range(2)
        if (dz, fy, fx) != (0, 0, 0)
    ]
    entries.sort(key=lambda e: (abs(e[0]) + e[1] + e[2], abs(e[0]), e))
    return entries


def layer_kernel(
    grid, shapes, res, qlt, qbt, lat, cosine, sine, ag, mg, kul, kub, vul, vub, wol, wob, gw, uw, dw, out,
    lat_all, gate_all, up_all, down_all, ql, qb, ktl, ktb, valt_l, valt_b, peak, total, acc_l, acc_b, att, term, inbox, kept,
    normed, hidden, inbox2, lat_recv, lat_send, lat_pair, recv, send, own_sem, pair_send, pair_recv,
):
    wide_z, wide_y, wide_x = grid
    n_sp = wide_z * wide_y * wide_x
    tokens, share, rope = shapes
    heads_l, heads_b = qlt.shape[0], qbt.shape[0]
    bf16, f32 = jnp.bfloat16, jnp.float32
    me = lax.axis_index("sp")
    core = lax.axis_index("tp")
    my_x = lax.rem(me, wide_x)
    my_y = lax.rem(me // wide_x, wide_y)
    my_z = me // (wide_x * wide_y)
    here = (my_z, my_y, my_x)
    strides = (wide_y * wide_x, wide_x, 1)
    Z, Y, X = 0, 1, 2
    flip_y = me + (1 - 2 * my_y) * strides[1]
    flip_x = me + (1 - 2 * my_x)
    ways = (
        (X, None, None, flip_x),
        (Y, None, None, flip_y),
        (Z, -1, my_z > 0, jnp.maximum(me - strides[0], 0)),
        (Z, 1, my_z < wide_z - 1, jnp.minimum(me + strides[0], n_sp - 1)),
    )

    barrier = pltpu.get_barrier_semaphore()
    for dim, sign, exists, where in ways:
        def greet(where=where):
            pl.semaphore_signal(barrier, inc=1, device_id={"sp": where})
        if exists is None:
            greet()
        else:
            pl.when(exists)(greet)
    pl.semaphore_signal(barrier, inc=1, device_id={"tp": 1 - core})
    ends = jnp.where(my_z > 0, 1, 0) + jnp.where(my_z < wide_z - 1, 1, 0)
    pl.semaphore_wait(barrier, 3 + ends)

    def wanted(order, origin, way):
        dim, sign, exists, _ = way
        place = order.index(dim)
        ok = origin[dim] == here[dim] if sign is None else sign * (here[dim] - origin[dim]) >= 0
        for later in order[place + 1:]:
            ok = jnp.logical_and(ok, origin[later] == here[later])
        return ok if exists is None else jnp.logical_and(ok, exists)

    def index_of(origin):
        return origin[0] * strides[0] + origin[1] * strides[1] + origin[2]

    gate_rows, units = gw.shape
    down_cols = dw.shape[1]
    cut = units // 4
    ORDER_A, ORDER_B, ORDER_C, ORDER_D = (Z, X, Y), (Z, Y, X), (X, Y, Z), (Y, X, Z)

    def gate_at(ref):
        return lambda i: ref.at[pl.ds(pl.multiple_of(i * gate_rows, gate_rows), gate_rows)]

    def down_at(k):
        return lambda i: down_all.at[
            pl.ds(k * cut, cut), pl.ds(pl.multiple_of(i * down_cols, down_cols), down_cols)
        ]

    parts = [
        (ORDER_A, gw, gate_at(gate_all)),
        (ORDER_B, uw, gate_at(up_all)),
    ] + [
        (order, dw.at[pl.ds(k * cut, cut)], down_at(k))
        for k, order in enumerate((ORDER_A, ORDER_B, ORDER_C, ORDER_D))
    ]

    def part_copy(p, w, i, mine):
        order, own, at = parts[p]
        return pltpu.make_async_remote_copy(
            src_ref=own if mine else at(i), dst_ref=at(i), send_sem=send.at[p, w, i],
            recv_sem=recv.at[p, i], device_id={"sp": ways[w][3]},
        )

    half = lat.shape[0] // 2
    first = pl.multiple_of(core * half, half)

    def lat_at(i):
        return lat_all.at[i, pl.ds(first, half)]

    def lat_copy(w, i, mine):
        return pltpu.make_async_remote_copy(
            src_ref=lat.at[pl.ds(first, half)] if mine else lat_at(i), dst_ref=lat_at(i),
            send_sem=lat_send.at[w, i], recv_sem=lat_recv.at[i], device_id={"sp": ways[w][3]},
        )

    def pair_lat(i):
        return pltpu.make_async_remote_copy(
            src_ref=lat_at(i), dst_ref=lat_at(i), send_sem=lat_pair.at[0, i],
            recv_sem=lat_pair.at[1, i], device_id={"tp": 1 - core},
        )

    def run(condition, action):
        if condition is None:
            action()
        else:
            pl.when(condition)(action)

    for w, way in enumerate(ways):
        run(way[2], lambda w=w: lat_copy(w, me, True).start())
    own = [pltpu.make_async_copy(lat, lat_all.at[me], own_sem.at[0])]
    for p, (_, src, at) in enumerate(parts):
        own.append(pltpu.make_async_copy(src, at(me), own_sem.at[1 + p]))
    for copy in own:
        copy.start()

    def send_own(w):
        for p in range(len(parts)):
            run(ways[w][2], lambda p=p: part_copy(p, w, me, True).start())

    send_own(0)

    table = hop_table(grid)
    codes = [((dz + wide_z - 1) * 2 + fy) * 2 + fx for dz, fy, fx in table]
    per = 4
    words = [
        sum(code << (7 * k) for k, code in enumerate(codes[at:at + per]))
        for at in range(0, len(codes), per)
    ]

    def origin_of(n):
        word = jnp.int32(words[0])
        for k in range(1, len(words)):
            word = jnp.where(n // per == k, jnp.int32(words[k]), word)
        rem = lax.rem(n, per)
        for k in range(1, per):
            word = jnp.where(rem >= k, word // 128, word)
        code = lax.rem(word, 128)
        dz = code // 4 - (wide_z - 1)
        fy = lax.rem(code // 2, 2)
        fx = lax.rem(code, 2)
        oz = my_z + dz
        oy = my_y + fy * (1 - 2 * my_y)
        ox = my_x + fx * (1 - 2 * my_x)
        return (oz, oy, ox), jnp.logical_and(oz >= 0, oz < wide_z)

    def lat_event(n, _):
        origin, valid = origin_of(n)

        @pl.when(valid)
        def _():
            i = index_of(origin)
            lat_copy(0, i, False).wait_recv()
            for w, way in enumerate(ways):
                run(wanted(ORDER_C, origin, way), lambda w=w: lat_copy(w, i, False).start())
            pair_lat(i).start()

        return 0

    def part_event(n, _):
        origin, valid = origin_of(n)

        @pl.when(valid)
        def _():
            i = index_of(origin)
            for p, (order, _, _) in enumerate(parts):
                part_copy(p, 0, i, False).wait_recv()
                for w, way in enumerate(ways):
                    run(wanted(order, origin, way), lambda p=p, w=w: part_copy(p, w, i, False).start())

        return 0

    count = len(table)
    early = sum(1 for dz, fy, fx in table if abs(dz) + fy + fx <= 2)
    lax.fori_loop(0, early, lat_event, 0)
    send_own(1)
    lax.fori_loop(early, count, lat_event, 0)
    send_own(2)
    send_own(3)
    half_rope = rope // 2
    for given, query in ((qlt, ql), (qbt, qb)):
        nope = given.shape[1] - rope
        for h in range(given.shape[0]):
            one = given[h, nope:nope + half_rope, :].astype(f32)
            two = given[h, nope + half_rope:, :].astype(f32)
            query[h, :nope, :] = given[h, :nope, :]
            query[h, nope:nope + half_rope, :] = (one * cosine[...] - two * sine[...]).astype(bf16)
            query[h, nope + half_rope:, :] = (one * sine[...] + two * cosine[...]).astype(bf16)
    for copy in own:
        copy.wait()

    def lat_arrived(i, _):
        pl.when(i != me)(lambda: pair_lat(i).wait_recv())
        return 0

    lax.fori_loop(0, n_sp, lat_arrived, 0)

    peak[...] = jnp.full(peak.shape, NEGATIVE, f32)
    total[...] = jnp.zeros(total.shape, f32)
    acc_l[...] = jnp.zeros(acc_l.shape, f32)
    acc_b[...] = jnp.zeros(acc_b.shape, f32)
    wide_l = kul.shape[0] // heads_l
    wide_b = kub.shape[0] // heads_b
    contract = (((1,), (1,)), ((), ()))
    contract_rows = (((0,), (0,)), ((), ()))

    def attend_block(j, masked):
        rows = lat_all[j, :tokens, :]
        rot = lat_all[j, tokens:, :]
        for ups, keys, heads, wide in ((kul, ktl, heads_l, wide_l), (kub, ktb, heads_b, wide_b)):
            made = lax.dot_general(ups[...], rows, contract, preferred_element_type=f32).astype(bf16)
            for h in range(heads):
                keys[h, :wide, :] = made[h * wide:(h + 1) * wide]
                keys[h, wide:, :] = rot
        for ups, held in ((vul, valt_l), (vub, valt_b)):
            held[...] = lax.dot_general(
                ups[...], rows, contract, preferred_element_type=f32
            ).astype(bf16)
        if masked:
            key_pos = lax.broadcasted_iota(jnp.int32, (tokens, tokens), 0)
            visible = key_pos <= lax.broadcasted_iota(jnp.int32, (tokens, tokens), 1)
        for g in range(heads_l + heads_b):
            if g < heads_l:
                h, query, keys, held, acc, wide = g, ql, ktl, valt_l, acc_l, wide_l
            else:
                h, query, keys, held, acc, wide = g - heads_l, qb, ktb, valt_b, acc_b, wide_b
            scores = lax.dot_general(
                keys[h], query[h], contract_rows, preferred_element_type=f32
            ) * (LOG2E * query.shape[1] ** (-0.5))
            if masked:
                scores = jnp.where(visible, scores, NEGATIVE)
            old = peak[g]
            new = jnp.maximum(old, jnp.max(scores, axis=0, keepdims=True))
            weights = jnp.exp2(scores - new)
            factor = jnp.exp2(old - new)
            peak[g] = new
            total[g] = total[g] * factor + jnp.sum(weights, axis=0, keepdims=True)
            acc[h] = acc[h] * factor + jnp.dot(
                held[h * wide:(h + 1) * wide, :], weights.astype(bf16), preferred_element_type=f32
            )

    def step(j, _):
        lax.fori_loop((j * early) // n_sp, ((j + 1) * early) // n_sp, part_event, 0)
        pl.when(j < me)(lambda: attend_block(j, False))
        return 0

    lax.fori_loop(0, n_sp, step, 0)
    attend_block(me, True)

    split = heads_l * wide_l
    for heads, wide, acc, base, col in (
        (heads_l, wide_l, acc_l, 0, 0), (heads_b, wide_b, acc_b, heads_l, split),
    ):
        together = wide_b // wide
        for h in range(0, heads, together):
            done = jnp.concatenate(
                [acc[h + k] / total[base + h + k] for k in range(together)], axis=0
            )
            att[:, col + h * wide:col + (h + together) * wide] = done.T.astype(bf16)

    features = out.shape[1]
    block = math.gcd(features, 512)

    def project(n, _):
        cols = pl.ds(pl.multiple_of(n * block, block), block)
        term[:, cols] = (
            jnp.dot(att[:, :split], wol[:, cols], preferred_element_type=f32)
            + jnp.dot(att[:, split:], wob[:, cols], preferred_element_type=f32)
        ).astype(bf16)
        return 0

    lax.fori_loop(0, features // block, project, 0)
    mine = pl.ds(pl.multiple_of(core * share, share), share)
    theirs = pl.ds(pl.multiple_of((1 - core) * share, share), share)

    def to_pair(k, src, dst):
        return pltpu.make_async_remote_copy(
            src_ref=src, dst_ref=dst, send_sem=pair_send.at[k], recv_sem=pair_recv.at[k],
            device_id={"tp": 1 - core},
        )

    heads_out = to_pair(0, term.at[theirs], inbox)
    heads_out.start()
    heads_out.wait_recv()
    rows_at_once = math.gcd(share, 16)

    def norms(n, _):
        rows = pl.ds(pl.multiple_of(n * rows_at_once, rows_at_once), rows_at_once)
        full = pl.ds(pl.multiple_of(core * share + n * rows_at_once, rows_at_once), rows_at_once)
        summed = term[full, :].astype(f32) + inbox[rows, :].astype(f32)
        branch = normalize(summed, ag[...])
        mixed = (res[rows, :].astype(f32) + branch).astype(bf16)
        kept[rows, :] = mixed
        normed[full, :] = normalize(mixed.astype(f32), mg[...]).astype(bf16)
        return 0

    lax.fori_loop(0, share // rows_at_once, norms, 0)
    rows_out = to_pair(1, normed.at[mine], normed.at[mine])
    rows_out.start()
    lax.fori_loop(early, count, part_event, 0)
    to_pair(1, normed.at[theirs], normed.at[theirs]).wait_recv()

    def feed(cols):
        gate = jnp.dot(normed[...], gate_all[:, cols], preferred_element_type=f32)
        up = jnp.dot(normed[...], up_all[:, cols], preferred_element_type=f32)
        hidden[:, cols] = (gate / (1.0 + jnp.exp(-gate)) * up).astype(bf16)

    span = 256

    def feed_loop(n, _):
        feed(pl.ds(pl.multiple_of(n * span, span), span))
        return 0

    lax.fori_loop(0, units // span, feed_loop, 0)
    if units % span:
        feed(pl.ds(units // span * span, units % span))
    heads_out.wait_send()
    wide_n = math.gcd(features, 256)

    def down(n, _):
        cols = pl.ds(pl.multiple_of(n * wide_n, wide_n), wide_n)
        term[:, cols] = jnp.dot(
            hidden[...], down_all[:, cols], preferred_element_type=f32
        ).astype(bf16)
        return 0

    lax.fori_loop(0, features // wide_n, down, 0)
    sums_out = to_pair(2, term.at[theirs], inbox2)
    sums_out.start()

    def sent(i, _):
        origin = (i // strides[0], lax.rem(i // strides[1], wide_y), lax.rem(i, wide_x))
        for w, way in enumerate(ways):
            run(wanted(ORDER_C, origin, way), lambda w=w: lat_copy(w, i, False).wait_send())
            for p, (order, _, _) in enumerate(parts):
                run(wanted(order, origin, way), lambda p=p, w=w: part_copy(p, w, i, False).wait_send())
        pl.when(i != me)(lambda: pair_lat(i).wait_send())
        return 0

    lax.fori_loop(0, n_sp, sent, 0)
    rows_out.wait_send()
    sums_out.wait_recv()

    def finish(n, _):
        rows = pl.ds(pl.multiple_of(n * rows_at_once, rows_at_once), rows_at_once)
        full = pl.ds(pl.multiple_of(core * share + n * rows_at_once, rows_at_once), rows_at_once)
        summed = term[full, :].astype(f32) + inbox2[rows, :].astype(f32)
        out[rows, :] = (kept[rows, :].astype(f32) + 0.5 * summed).astype(bf16)
        return 0

    lax.fori_loop(0, share // rows_at_once, finish, 0)
    sums_out.wait_send()


def fused_shards(
    grid, residual_in, query_lean, query_broad, latent, rope_key, latent_gain, key_up_lean,
    key_up_broad, value_up_lean, value_up_broad, out_lean, out_broad, attn_gain, mlp_gain,
    gate_weight, up_weight, down_weight,
):
    bf16, f32 = jnp.bfloat16, jnp.float32
    tokens = query_lean.shape[0]
    share, features = residual_in.shape
    rank = latent.shape[1]
    rope = rope_key.shape[1]
    n_sp = lax.axis_size("sp")
    positions = lax.axis_index("sp") * tokens + jnp.arange(tokens, dtype=jnp.int32)

    ql, qb = (jnp.transpose(query, (1, 2, 0)) for query in (query_lean, query_broad))
    freqs = THETA ** (-2.0 * jnp.arange(rope // 2, dtype=f32) / rope)
    angle = freqs[:, None] * positions.astype(f32)[None, :]
    lat = normalize(latent.astype(f32), latent_gain).astype(bf16)
    rot_key = rotate(rope_key.astype(f32), positions).astype(bf16)
    lat = jnp.concatenate([lat, rot_key.T], axis=0)
    kul = key_up_lean.reshape(rank, -1).T
    kub = key_up_broad.reshape(rank, -1).T
    vul = value_up_lean.reshape(rank, -1).T
    vub = value_up_broad.reshape(rank, -1).T
    wol = out_lean.reshape(-1, features)
    wob = out_broad.reshape(-1, features)
    heads = ql.shape[0] + qb.shape[0]
    units = gate_weight.shape[1]
    wide_b = value_up_broad.shape[2]
    vmem = pl.BlockSpec(memory_space=pltpu.VMEM)
    args = (
        residual_in, ql, qb, lat, jnp.cos(angle), jnp.sin(angle), attn_gain[None], mlp_gain[None],
        kul, kub, vul, vub, wol, wob,
        gate_weight, up_weight, down_weight,
    )
    dma = pltpu.SemaphoreType.DMA
    return pl.pallas_call(
        functools.partial(layer_kernel, grid, (tokens, share, rope)),
        out_shape=jax.ShapeDtypeStruct((share, features), bf16),
        in_specs=[vmem] * len(args),
        out_specs=vmem,
        scratch_shapes=[
            pltpu.VMEM((n_sp, tokens + rope, rank), bf16),
            pltpu.VMEM((features, units), bf16),
            pltpu.VMEM((features, units), bf16),
            pltpu.VMEM((units, features), bf16),
            pltpu.VMEM(ql.shape, bf16),
            pltpu.VMEM(qb.shape, bf16),
            pltpu.VMEM(ql.shape, bf16),
            pltpu.VMEM(qb.shape, bf16),
            pltpu.VMEM((vul.shape[0], tokens), bf16),
            pltpu.VMEM((vub.shape[0], tokens), bf16),
            pltpu.VMEM((heads, 1, tokens), f32),
            pltpu.VMEM((heads, 1, tokens), f32),
            pltpu.VMEM((ql.shape[0], value_up_lean.shape[2], tokens), f32),
            pltpu.VMEM((qb.shape[0], wide_b, tokens), f32),
            pltpu.VMEM((tokens, vul.shape[0] + vub.shape[0]), bf16),
            pltpu.VMEM((tokens, features), bf16),
            pltpu.VMEM((share, features), bf16),
            pltpu.VMEM((share, features), bf16),
            pltpu.VMEM((tokens, features), bf16),
            pltpu.VMEM((tokens, units), bf16),
            pltpu.VMEM((share, features), bf16),
            dma((n_sp,)),
            dma((4, n_sp)),
            dma((2, n_sp)),
            dma((6, n_sp)),
            dma((6, 4, n_sp)),
            dma((7,)),
            dma((3,)),
            dma((3,)),
        ],
        compiler_params=pltpu.CompilerParams(
            collective_id=0, has_side_effects=True, vmem_limit_bytes=62 * 2**20
        ),
    )(*args)


def fits(grid, mesh, args):
    if grid is None or mesh.shape["tp"] != 2 or grid[1] != 2 or grid[2] != 2 or grid[0] > 8:
        return False
    n_sp = mesh.shape["sp"]
    tokens = args[1].shape[0] // n_sp
    share = tokens // 2
    units = args[14].shape[1] // 2
    heads_l, heads_b = args[6].shape[1] // 2, args[7].shape[1] // 2
    wide_l, wide_b = args[6].shape[2], args[7].shape[2]
    rope = args[4].shape[1]
    return (
        tokens % 128 == 0 and tokens <= 256 and share % 16 == 0 and units % 128 == 0
        and units % 64 == 0 and heads_l % 2 == 0 and 2 * wide_l == wide_b and wide_b % 128 == 0
        and args[3].shape[1] == tokens and rope % 32 == 0 and (tokens + rope) % 32 == 0
        and heads_b > 0 and args[8].shape[2] == wide_l and args[9].shape[2] == wide_b
        and (args[14].shape[0] // n_sp) % 16 == 0 and (args[16].shape[1] // n_sp) % 128 == 0
    )


def solution(mesh):
    in_specs = (
        P(("sp", "tp"), None),
        P("sp", "tp", None),
        P("sp", "tp", None),
        P("sp", None),
        P("sp", None),
        P(),
        P(None, "tp", None),
        P(None, "tp", None),
        P(None, "tp", None),
        P(None, "tp", None),
        P("tp", None, None),
        P("tp", None, None),
        P(),
        P(),
        P("sp", "tp"),
        P("sp", "tp"),
        P("tp", "sp"),
    )
    out_specs = P(("sp", "tp"), None)
    grid = grid_of(mesh)

    def layer(*args):
        body = functools.partial(fused_shards, grid) if fits(grid, mesh, args) else shards
        return jax.shard_map(
            body, mesh=mesh, in_specs=in_specs, out_specs=out_specs, check_vma=False
        )(*args)

    return layer
```

```python
import functools
import math

import jax
import jax.numpy as jnp
from jax import lax
from jax.experimental import pallas as pl
from jax.experimental.pallas import tpu as pltpu
from jax.sharding import PartitionSpec as P

THETA = 10000.0
EPS = 1e-06
NEGATIVE = -1e30


def rotate(values, positions):
    width = values.shape[-1]
    half = width // 2
    freqs = THETA ** (-2.0 * jnp.arange(half, dtype=jnp.float32) / width)
    angle = positions.astype(jnp.float32)[:, None] * freqs[None, :]
    cosine = jnp.cos(angle)
    sine = jnp.sin(angle)
    if values.ndim == 3:
        cosine = cosine[:, None, :]
        sine = sine[:, None, :]
    first = values[..., :half]
    second = values[..., half:]
    return jnp.concatenate(
        [first * cosine - second * sine, first * sine + second * cosine], axis=-1
    )


def normalize(values, gain):
    return values * lax.rsqrt(jnp.mean(values * values, axis=-1, keepdims=True) + EPS) * gain


def block_keys(weights, latent_rows):
    projected = []
    for key_up, value_up in weights:
        keys = jnp.einsum(
            "kr,rhd->khd", latent_rows, key_up, preferred_element_type=jnp.float32
        ).astype(jnp.bfloat16)
        values = jnp.einsum(
            "kr,rhd->khd", latent_rows, value_up, preferred_element_type=jnp.float32
        ).astype(jnp.bfloat16)
        projected.append((keys, values))
    return projected


def attend(carry, queries, projected, rotated_rows, key_pos, query_pos):
    updated = []
    visible = key_pos[None, :] <= query_pos[:, None]
    for state, query, pair in zip(carry, queries, projected):
        query_nope, query_rot, scale = query
        keys, values = pair
        peak, total, accum = state
        scores = (
            jnp.einsum("qhd,khd->hqk", query_nope, keys, preferred_element_type=jnp.float32)
            + jnp.einsum("qhr,kr->hqk", query_rot, rotated_rows, preferred_element_type=jnp.float32)
        ) * scale
        scores = jnp.where(visible[None], scores, NEGATIVE)
        new_peak = jnp.maximum(peak, jnp.max(scores, axis=-1))
        weights = jnp.where(visible[None], jnp.exp(scores - new_peak[..., None]), 0.0)
        factor = jnp.exp(peak - new_peak)
        total = total * factor + jnp.sum(weights, axis=-1)
        accum = accum * factor[..., None] + jnp.einsum(
            "hqk,khv->hqv", weights.astype(jnp.bfloat16), values, preferred_element_type=jnp.float32
        )
        updated.append((new_peak, total, accum))
    return tuple(updated)


def fold_piece(carry, latent_piece, rotated_piece, piece_pos, weights, segments):
    count = latent_piece.shape[0]
    block = math.gcd(count, 1024)
    last_all = segments[0][1][-1]

    def one_block(index, state):
        lat_rows = lax.dynamic_slice_in_dim(latent_piece, index * block, block, 0)
        rot_rows = lax.dynamic_slice_in_dim(rotated_piece, index * block, block, 0)
        pos_rows = lax.dynamic_slice_in_dim(piece_pos, index * block, block, 0)
        first_key = jnp.min(pos_rows)

        def work(inner):
            projected = block_keys(weights, lat_rows)
            results = []
            for inner_seg, segment in zip(inner, segments):
                queries, seg_pos = segment
                results.append(
                    lax.cond(
                        first_key <= seg_pos[-1],
                        lambda held, queries=queries, seg_pos=seg_pos: attend(
                            held, queries, projected, rot_rows, pos_rows, seg_pos
                        ),
                        lambda held: held,
                        inner_seg,
                    )
                )
            return tuple(results)

        return lax.cond(first_key <= last_all, work, lambda inner: inner, state)

    return lax.fori_loop(0, count // block, one_block, carry)


def shards(
    residual_in,
    query_lean,
    query_broad,
    latent,
    rope_key,
    latent_gain,
    key_up_lean,
    key_up_broad,
    value_up_lean,
    value_up_broad,
    out_lean,
    out_broad,
    attn_gain,
    mlp_gain,
    gate_weight,
    up_weight,
    down_weight,
):
    tokens_here = query_lean.shape[0]
    n_tp = lax.axis_size("tp")
    share = tokens_here // n_tp
    sp_index = lax.axis_index("sp")
    first = sp_index * tokens_here
    query_pos = first + jnp.arange(tokens_here, dtype=jnp.int32)
    rope_width = rope_key.shape[1]
    weights = ((key_up_lean, value_up_lean), (key_up_broad, value_up_broad))
    segment_rows = (query_lean, query_broad, query_pos)
    segments = []
    initial = []
    lean_rows, broad_rows, seg_pos = segment_rows
    queries = []
    states = []
    for query, value_up in ((lean_rows, value_up_lean), (broad_rows, value_up_broad)):
        nope = query.shape[2] - rope_width
        query_rot = rotate(query[:, :, nope:].astype(jnp.float32), seg_pos).astype(jnp.bfloat16)
        queries.append((query[:, :, :nope], query_rot, query.shape[2] ** (-0.5)))
        heads = query.shape[1]
        rows = query.shape[0]
        states.append(
            (
                jnp.full((heads, rows), NEGATIVE, jnp.float32),
                jnp.zeros((heads, rows), jnp.float32),
                jnp.zeros((heads, rows, value_up.shape[2]), jnp.float32),
            )
        )
    segments.append((tuple(queries), seg_pos))
    initial.append(tuple(states))
    segments = tuple(segments)
    initial = tuple(initial)
    sent_latent = normalize(latent.astype(jnp.float32), latent_gain).astype(jnp.bfloat16)
    sent_rot = rotate(rope_key.astype(jnp.float32), query_pos).astype(jnp.bfloat16)
    pieces = (
        lax.all_gather(sent_latent, "sp", axis=0, tiled=True),
        lax.all_gather(sent_rot, "sp", axis=0, tiled=True),
    )
    piece_pos = jnp.arange(pieces[0].shape[0], dtype=jnp.int32)
    folded = fold_piece(initial, pieces[0], pieces[1], piece_pos, weights, segments)
    results = [
        [(accum / total[..., None]).astype(jnp.bfloat16) for peak, total, accum in seg_state]
        for seg_state in folded
    ]
    attended = results[0]
    term = jnp.zeros((share * lax.axis_size("tp"), out_lean.shape[2]), jnp.float32)
    for rows_all, weight in ((attended[0], out_lean), (attended[1], out_broad)):
        rows = rows_all
        term = term + jnp.einsum("hqv,hvd->qd", rows, weight, preferred_element_type=jnp.float32)
    head_sum = lax.psum_scatter(
        term.astype(jnp.bfloat16), "tp", scatter_dimension=0, tiled=True
    ).astype(jnp.float32)
    branch = normalize(head_sum, attn_gain)
    kept = (residual_in.astype(jnp.float32) + branch).astype(jnp.bfloat16)
    normed = normalize(kept.astype(jnp.float32), mlp_gain).astype(jnp.bfloat16)
    whole_normed = lax.all_gather(normed, "tp", axis=0, tiled=True)
    gate_whole, up_whole, down_whole = (
        lax.all_gather(gate_weight, "sp", axis=0, tiled=True),
        lax.all_gather(up_weight, "sp", axis=0, tiled=True),
        lax.all_gather(down_weight, "sp", axis=1, tiled=True),
    )
    gate = jnp.dot(whole_normed, gate_whole, preferred_element_type=jnp.float32)
    up = jnp.dot(whole_normed, up_whole, preferred_element_type=jnp.float32)
    hidden = (jax.nn.silu(gate) * up).astype(jnp.bfloat16)
    rows = hidden
    channel_sum = lax.psum_scatter(
        jnp.dot(rows, down_whole, preferred_element_type=jnp.float32).astype(jnp.bfloat16),
        "tp",
        scatter_dimension=0,
        tiled=True,
    ).astype(jnp.float32)
    return (kept.astype(jnp.float32) + 0.5 * channel_sum).astype(jnp.bfloat16)


LOG2E = math.log2(math.e)


def grid_of(mesh):
    n_sp, n_tp = mesh.shape["sp"], mesh.shape["tp"]
    devices = mesh.devices.reshape(n_sp, n_tp)
    try:
        places = [tuple(device.coords) for device in devices[:, 0]]
        partners = [tuple(device.coords) for device in devices[:, -1]]
    except Exception:
        return (n_sp // 4, 2, 2) if n_sp % 4 == 0 else None
    if places != partners:
        return None
    low = [min(place[k] for place in places) for k in range(3)]
    sizes = [max(place[k] for place in places) - low[k] + 1 for k in range(3)]
    wide_z, wide_y, wide_x = sizes[2], sizes[1], sizes[0]
    if wide_z * wide_y * wide_x != n_sp:
        return None
    for index, place in enumerate(places):
        x, y, z = (place[k] - low[k] for k in range(3))
        if (z * wide_y + y) * wide_x + x != index:
            return None
    return wide_z, wide_y, wide_x


def hop_table(grid):
    wide_z = grid[0]
    entries = [
        (dz, fy, fx)
        for dz in range(1 - wide_z, wide_z)
        for fy in range(2)
        for fx in range(2)
        if (dz, fy, fx) != (0, 0, 0)
    ]
    entries.sort(key=lambda e: (abs(e[0]) + e[1] + e[2], abs(e[0]), e))
    return entries


def layer_kernel(
    grid, shapes, res_in, qlt, qbt, lat, cosine, sine, ag, mg, kul, kub, vul, vub, wol_in, wob_in, gw, uw, dw, out,
    lat_all, gate_all, up_all, down_all, ql, qb, ktl, ktb, valt_l, valt_b, peak, total, acc_l, acc_b, att, term, inbox, kept,
    normed, hidden, inbox2, wol, wob, res, lat_recv, lat_send, lat_pair, recv, send, own_sem, pair_send, pair_recv,
):
    wide_z, wide_y, wide_x = grid
    n_sp = wide_z * wide_y * wide_x
    tokens, share, rope = shapes
    heads_l, heads_b = qlt.shape[0], qbt.shape[0]
    bf16, f32 = jnp.bfloat16, jnp.float32
    me = lax.axis_index("sp")
    core = lax.axis_index("tp")
    my_x = lax.rem(me, wide_x)
    my_y = lax.rem(me // wide_x, wide_y)
    my_z = me // (wide_x * wide_y)
    here = (my_z, my_y, my_x)
    strides = (wide_y * wide_x, wide_x, 1)
    Z, Y, X = 0, 1, 2
    flip_y = me + (1 - 2 * my_y) * strides[1]
    flip_x = me + (1 - 2 * my_x)
    ways = (
        (X, None, None, flip_x),
        (Y, None, None, flip_y),
        (Z, -1, my_z > 0, jnp.maximum(me - strides[0], 0)),
        (Z, 1, my_z < wide_z - 1, jnp.minimum(me + strides[0], n_sp - 1)),
    )

    barrier = pltpu.get_barrier_semaphore()
    for dim, sign, exists, where in ways:
        def greet(where=where):
            pl.semaphore_signal(barrier, inc=1, device_id={"sp": where})
        if exists is None:
            greet()
        else:
            pl.when(exists)(greet)
    pl.semaphore_signal(barrier, inc=1, device_id={"tp": 1 - core})
    ends = jnp.where(my_z > 0, 1, 0) + jnp.where(my_z < wide_z - 1, 1, 0)
    pl.semaphore_wait(barrier, 3 + ends)

    def wanted(order, origin, way):
        dim, sign, exists, _ = way
        place = order.index(dim)
        ok = origin[dim] == here[dim] if sign is None else sign * (here[dim] - origin[dim]) >= 0
        for later in order[place + 1:]:
            ok = jnp.logical_and(ok, origin[later] == here[later])
        return ok if exists is None else jnp.logical_and(ok, exists)

    def index_of(origin):
        return origin[0] * strides[0] + origin[1] * strides[1] + origin[2]

    gate_rows, units = gw.shape
    down_cols = dw.shape[1]
    cut = units // 4
    ORDER_A, ORDER_B, ORDER_C, ORDER_D = (Z, X, Y), (Z, Y, X), (X, Y, Z), (Y, X, Z)

    def gate_at(ref):
        return lambda i: ref.at[pl.ds(pl.multiple_of(i * gate_rows, gate_rows), gate_rows)]

    def down_at(k):
        return lambda i: down_all.at[
            pl.ds(k * cut, cut), pl.ds(pl.multiple_of(i * down_cols, down_cols), down_cols)
        ]

    parts = [
        (ORDER_A, gw, gate_at(gate_all)),
        (ORDER_B, uw, gate_at(up_all)),
    ] + [
        (order, dw.at[pl.ds(k * cut, cut)], down_at(k))
        for k, order in enumerate((ORDER_A, ORDER_B, ORDER_C, ORDER_D))
    ]

    def part_copy(p, w, i, mine):
        order, own, at = parts[p]
        return pltpu.make_async_remote_copy(
            src_ref=own if mine else at(i), dst_ref=at(i), send_sem=send.at[p, w, i],
            recv_sem=recv.at[p, i], device_id={"sp": ways[w][3]},
        )

    half = lat.shape[0] // 2
    first = pl.multiple_of(core * half, half)

    def lat_at(i):
        return lat_all.at[i, pl.ds(first, half)]

    def lat_copy(w, i, mine):
        return pltpu.make_async_remote_copy(
            src_ref=lat.at[pl.ds(first, half)] if mine else lat_at(i), dst_ref=lat_at(i),
            send_sem=lat_send.at[w, i], recv_sem=lat_recv.at[i], device_id={"sp": ways[w][3]},
        )

    def pair_lat(i):
        return pltpu.make_async_remote_copy(
            src_ref=lat_at(i), dst_ref=lat_at(i), send_sem=lat_pair.at[0, i],
            recv_sem=lat_pair.at[1, i], device_id={"tp": 1 - core},
        )

    def run(condition, action):
        if condition is None:
            action()
        else:
            pl.when(condition)(action)

    for w, way in enumerate(ways):
        run(way[2], lambda w=w: lat_copy(w, me, True).start())
    own = [pltpu.make_async_copy(lat, lat_all.at[me], own_sem.at[0])]
    for p, (_, src, at) in enumerate(parts):
        own.append(pltpu.make_async_copy(src, at(me), own_sem.at[1 + p]))
    fetch = [
        pltpu.make_async_copy(src, dst, own_sem.at[1 + len(parts) + k])
        for k, (src, dst) in enumerate(((wol_in, wol), (wob_in, wob), (res_in, res)))
    ]
    for copy in own + fetch:
        copy.start()

    def send_own(w):
        for p in range(len(parts)):
            run(ways[w][2], lambda p=p: part_copy(p, w, me, True).start())

    send_own(0)

    table = hop_table(grid)
    codes = [((dz + wide_z - 1) * 2 + fy) * 2 + fx for dz, fy, fx in table]
    per = 4
    words = [
        sum(code << (7 * k) for k, code in enumerate(codes[at:at + per]))
        for at in range(0, len(codes), per)
    ]

    def origin_of(n):
        word = jnp.int32(words[0])
        for k in range(1, len(words)):
            word = jnp.where(n // per == k, jnp.int32(words[k]), word)
        rem = lax.rem(n, per)
        for k in range(1, per):
            word = jnp.where(rem >= k, word // 128, word)
        code = lax.rem(word, 128)
        dz = code // 4 - (wide_z - 1)
        fy = lax.rem(code // 2, 2)
        fx = lax.rem(code, 2)
        oz = my_z + dz
        oy = my_y + fy * (1 - 2 * my_y)
        ox = my_x + fx * (1 - 2 * my_x)
        return (oz, oy, ox), jnp.logical_and(oz >= 0, oz < wide_z)

    def lat_event(n, _):
        origin, valid = origin_of(n)

        @pl.when(valid)
        def _():
            i = index_of(origin)
            lat_copy(0, i, False).wait_recv()
            for w, way in enumerate(ways):
                run(wanted(ORDER_C, origin, way), lambda w=w: lat_copy(w, i, False).start())
            pair_lat(i).start()

        return 0

    def part_event(n, group):
        origin, valid = origin_of(n)

        @pl.when(valid)
        def _():
            i = index_of(origin)
            for p in group:
                part_copy(p, 0, i, False).wait_recv()
                for w, way in enumerate(ways):
                    run(
                        wanted(parts[p][0], origin, way),
                        lambda p=p, w=w: part_copy(p, w, i, False).start(),
                    )

    def events(low, high, group):
        def body(n, _):
            part_event(n, group)
            return 0

        lax.fori_loop(low, high, body, 0)

    soon, late = (0, 1, 4, 5), (2, 3)

    count = len(table)
    early = sum(1 for dz, fy, fx in table if abs(dz) + fy + fx <= 2)
    lax.fori_loop(0, early, lat_event, 0)
    send_own(1)
    lax.fori_loop(early, count, lat_event, 0)
    send_own(2)
    send_own(3)
    half_rope = rope // 2
    for given, query in ((qlt, ql), (qbt, qb)):
        nope = given.shape[1] - rope
        for h in range(given.shape[0]):
            one = given[h, nope:nope + half_rope, :].astype(f32)
            two = given[h, nope + half_rope:, :].astype(f32)
            query[h, :nope, :] = given[h, :nope, :]
            query[h, nope:nope + half_rope, :] = (one * cosine[...] - two * sine[...]).astype(bf16)
            query[h, nope + half_rope:, :] = (one * sine[...] + two * cosine[...]).astype(bf16)
    for copy in own:
        copy.wait()

    def lat_arrived(i, _):
        pl.when(i != me)(lambda: pair_lat(i).wait_recv())
        return 0

    lax.fori_loop(0, n_sp, lat_arrived, 0)

    peak[...] = jnp.full(peak.shape, NEGATIVE, f32)
    total[...] = jnp.zeros(total.shape, f32)
    acc_l[...] = jnp.zeros(acc_l.shape, f32)
    acc_b[...] = jnp.zeros(acc_b.shape, f32)
    wide_l = kul.shape[0] // heads_l
    wide_b = kub.shape[0] // heads_b
    contract = (((1,), (1,)), ((), ()))
    contract_rows = (((0,), (0,)), ((), ()))

    def attend_block(j, masked):
        rows = lat_all[j, :tokens, :]
        rot = lat_all[j, tokens:, :]
        for ups, keys, heads, wide in ((kul, ktl, heads_l, wide_l), (kub, ktb, heads_b, wide_b)):
            made = lax.dot_general(ups[...], rows, contract, preferred_element_type=f32).astype(bf16)
            for h in range(heads):
                keys[h, :wide, :] = made[h * wide:(h + 1) * wide]
                keys[h, wide:, :] = rot
        for ups, held in ((vul, valt_l), (vub, valt_b)):
            held[...] = lax.dot_general(
                ups[...], rows, contract, preferred_element_type=f32
            ).astype(bf16)
        if masked:
            key_pos = lax.broadcasted_iota(jnp.int32, (tokens, tokens), 0)
            visible = key_pos <= lax.broadcasted_iota(jnp.int32, (tokens, tokens), 1)
        for g in range(heads_l + heads_b):
            if g < heads_l:
                h, query, keys, held, acc, wide = g, ql, ktl, valt_l, acc_l, wide_l
            else:
                h, query, keys, held, acc, wide = g - heads_l, qb, ktb, valt_b, acc_b, wide_b
            scores = lax.dot_general(
                keys[h], query[h], contract_rows, preferred_element_type=f32
            ) * (LOG2E * query.shape[1] ** (-0.5))
            if masked:
                scores = jnp.where(visible, scores, NEGATIVE)
            old = peak[g]
            new = jnp.maximum(old, jnp.max(scores, axis=0, keepdims=True))
            weights = jnp.exp2(scores - new)
            factor = jnp.exp2(old - new)
            peak[g] = new
            total[g] = total[g] * factor + jnp.sum(weights, axis=0, keepdims=True)
            acc[h] = acc[h] * factor + jnp.dot(
                held[h * wide:(h + 1) * wide, :], weights.astype(bf16), preferred_element_type=f32
            )

    def step(j, _):
        events((j * early) // n_sp, ((j + 1) * early) // n_sp, soon)
        pl.when(j < me)(lambda: attend_block(j, False))
        return 0

    lax.fori_loop(0, n_sp, step, 0)
    attend_block(me, True)

    split = heads_l * wide_l
    for heads, wide, acc, base, col in (
        (heads_l, wide_l, acc_l, 0, 0), (heads_b, wide_b, acc_b, heads_l, split),
    ):
        together = wide_b // wide
        for h in range(0, heads, together):
            done = jnp.concatenate(
                [acc[h + k] / total[base + h + k] for k in range(together)], axis=0
            )
            att[:, col + h * wide:col + (h + together) * wide] = done.T.astype(bf16)

    features = out.shape[1]
    block = math.gcd(features, 512)

    for copy in fetch:
        copy.wait()

    def project(n, _):
        cols = pl.ds(pl.multiple_of(n * block, block), block)
        term[:, cols] = (
            jnp.dot(att[:, :split], wol[:, cols], preferred_element_type=f32)
            + jnp.dot(att[:, split:], wob[:, cols], preferred_element_type=f32)
        ).astype(bf16)
        return 0

    lax.fori_loop(0, features // block, project, 0)
    mine = pl.ds(pl.multiple_of(core * share, share), share)
    theirs = pl.ds(pl.multiple_of((1 - core) * share, share), share)

    def to_pair(k, src, dst):
        return pltpu.make_async_remote_copy(
            src_ref=src, dst_ref=dst, send_sem=pair_send.at[k], recv_sem=pair_recv.at[k],
            device_id={"tp": 1 - core},
        )

    heads_out = to_pair(0, term.at[theirs], inbox)
    heads_out.start()
    heads_out.wait_recv()
    rows_at_once = math.gcd(share, 16)

    def norms(n, _):
        rows = pl.ds(pl.multiple_of(n * rows_at_once, rows_at_once), rows_at_once)
        full = pl.ds(pl.multiple_of(core * share + n * rows_at_once, rows_at_once), rows_at_once)
        summed = term[full, :].astype(f32) + inbox[rows, :].astype(f32)
        branch = normalize(summed, ag[...])
        mixed = (res[rows, :].astype(f32) + branch).astype(bf16)
        kept[rows, :] = mixed
        normed[full, :] = normalize(mixed.astype(f32), mg[...]).astype(bf16)
        return 0

    lax.fori_loop(0, share // rows_at_once, norms, 0)
    rows_out = to_pair(1, normed.at[mine], normed.at[mine])
    rows_out.start()
    behind = min(early, count - early)

    def both_groups(n, _):
        part_event(n, soon)
        part_event(n - behind, late)
        return 0

    events(0, early - behind, late)
    lax.fori_loop(early, count, both_groups, 0)
    to_pair(1, normed.at[theirs], normed.at[theirs]).wait_recv()

    def feed(cols):
        gate = jnp.dot(normed[...], gate_all[:, cols], preferred_element_type=f32)
        up = jnp.dot(normed[...], up_all[:, cols], preferred_element_type=f32)
        hidden[:, cols] = (gate / (1.0 + jnp.exp(-gate)) * up).astype(bf16)

    span = 256
    chunks = units // span
    left = count - behind

    def feed_loop(n, _):
        events(left + (n * behind) // chunks, left + ((n + 1) * behind) // chunks, late)
        feed(pl.ds(pl.multiple_of(n * span, span), span))
        return 0

    lax.fori_loop(0, chunks, feed_loop, 0)
    if units % span:
        feed(pl.ds(units // span * span, units % span))
    heads_out.wait_send()
    wide_n = math.gcd(features, 256)

    def down(n, _):
        cols = pl.ds(pl.multiple_of(n * wide_n, wide_n), wide_n)
        term[:, cols] = jnp.dot(
            hidden[...], down_all[:, cols], preferred_element_type=f32
        ).astype(bf16)
        return 0

    lax.fori_loop(0, features // wide_n, down, 0)
    sums_out = to_pair(2, term.at[theirs], inbox2)
    sums_out.start()

    def sent(i, _):
        origin = (i // strides[0], lax.rem(i // strides[1], wide_y), lax.rem(i, wide_x))
        for w, way in enumerate(ways):
            run(wanted(ORDER_C, origin, way), lambda w=w: lat_copy(w, i, False).wait_send())
            for p, (order, _, _) in enumerate(parts):
                run(wanted(order, origin, way), lambda p=p, w=w: part_copy(p, w, i, False).wait_send())
        pl.when(i != me)(lambda: pair_lat(i).wait_send())
        return 0

    lax.fori_loop(0, n_sp, sent, 0)
    rows_out.wait_send()
    sums_out.wait_recv()

    def finish(n, _):
        rows = pl.ds(pl.multiple_of(n * rows_at_once, rows_at_once), rows_at_once)
        full = pl.ds(pl.multiple_of(core * share + n * rows_at_once, rows_at_once), rows_at_once)
        summed = term[full, :].astype(f32) + inbox2[rows, :].astype(f32)
        out[rows, :] = (kept[rows, :].astype(f32) + 0.5 * summed).astype(bf16)
        return 0

    lax.fori_loop(0, share // rows_at_once, finish, 0)
    sums_out.wait_send()


def fused_shards(
    grid, residual_in, query_lean, query_broad, latent, rope_key, latent_gain, key_up_lean,
    key_up_broad, value_up_lean, value_up_broad, out_lean, out_broad, attn_gain, mlp_gain,
    gate_weight, up_weight, down_weight,
):
    bf16, f32 = jnp.bfloat16, jnp.float32
    tokens = query_lean.shape[0]
    share, features = residual_in.shape
    rank = latent.shape[1]
    rope = rope_key.shape[1]
    n_sp = lax.axis_size("sp")
    positions = lax.axis_index("sp") * tokens + jnp.arange(tokens, dtype=jnp.int32)

    ql, qb = (jnp.transpose(query, (1, 2, 0)) for query in (query_lean, query_broad))
    freqs = THETA ** (-2.0 * jnp.arange(rope // 2, dtype=f32) / rope)
    angle = freqs[:, None] * positions.astype(f32)[None, :]
    lat = normalize(latent.astype(f32), latent_gain).astype(bf16)
    rot_key = rotate(rope_key.astype(f32), positions).astype(bf16)
    lat = jnp.concatenate([lat, rot_key.T], axis=0)
    kul = key_up_lean.reshape(rank, -1).T
    kub = key_up_broad.reshape(rank, -1).T
    vul = value_up_lean.reshape(rank, -1).T
    vub = value_up_broad.reshape(rank, -1).T
    wol = out_lean.reshape(-1, features)
    wob = out_broad.reshape(-1, features)
    heads = ql.shape[0] + qb.shape[0]
    units = gate_weight.shape[1]
    wide_b = value_up_broad.shape[2]
    vmem = pl.BlockSpec(memory_space=pltpu.VMEM)
    args = (
        residual_in, ql, qb, lat, jnp.cos(angle), jnp.sin(angle), attn_gain[None], mlp_gain[None],
        kul, kub, vul, vub, wol, wob,
        gate_weight, up_weight, down_weight,
    )
    dma = pltpu.SemaphoreType.DMA
    return pl.pallas_call(
        functools.partial(layer_kernel, grid, (tokens, share, rope)),
        out_shape=jax.ShapeDtypeStruct((share, features), bf16),
        in_specs=[
            pl.BlockSpec(memory_space=pl.ANY) if k in (0, 12, 13) else vmem for k in range(len(args))
        ],
        out_specs=vmem,
        scratch_shapes=[
            pltpu.VMEM((n_sp, tokens + rope, rank), bf16),
            pltpu.VMEM((features, units), bf16),
            pltpu.VMEM((features, units), bf16),
            pltpu.VMEM((units, features), bf16),
            pltpu.VMEM(ql.shape, bf16),
            pltpu.VMEM(qb.shape, bf16),
            pltpu.VMEM(ql.shape, bf16),
            pltpu.VMEM(qb.shape, bf16),
            pltpu.VMEM((vul.shape[0], tokens), bf16),
            pltpu.VMEM((vub.shape[0], tokens), bf16),
            pltpu.VMEM((heads, 1, tokens), f32),
            pltpu.VMEM((heads, 1, tokens), f32),
            pltpu.VMEM((ql.shape[0], value_up_lean.shape[2], tokens), f32),
            pltpu.VMEM((qb.shape[0], wide_b, tokens), f32),
            pltpu.VMEM((tokens, vul.shape[0] + vub.shape[0]), bf16),
            pltpu.VMEM((tokens, features), bf16),
            pltpu.VMEM((share, features), bf16),
            pltpu.VMEM((share, features), bf16),
            pltpu.VMEM((tokens, features), bf16),
            pltpu.VMEM((tokens, units), bf16),
            pltpu.VMEM((share, features), bf16),
            pltpu.VMEM(wol.shape, bf16),
            pltpu.VMEM(wob.shape, bf16),
            pltpu.VMEM(residual_in.shape, bf16),
            dma((n_sp,)),
            dma((4, n_sp)),
            dma((2, n_sp)),
            dma((6, n_sp)),
            dma((6, 4, n_sp)),
            dma((10,)),
            dma((3,)),
            dma((3,)),
        ],
        compiler_params=pltpu.CompilerParams(
            collective_id=0, has_side_effects=True, vmem_limit_bytes=62 * 2**20
        ),
    )(*args)


def fits(grid, mesh, args):
    if grid is None or mesh.shape["tp"] != 2 or grid[1] != 2 or grid[2] != 2 or grid[0] > 8:
        return False
    n_sp = mesh.shape["sp"]
    tokens = args[1].shape[0] // n_sp
    share = tokens // 2
    units = args[14].shape[1] // 2
    heads_l, heads_b = args[6].shape[1] // 2, args[7].shape[1] // 2
    wide_l, wide_b = args[6].shape[2], args[7].shape[2]
    rope = args[4].shape[1]
    return (
        tokens % 128 == 0 and tokens <= 256 and share % 16 == 0 and units >= 256
        and units % 64 == 0 and heads_l % 2 == 0 and 2 * wide_l == wide_b and wide_b % 128 == 0
        and args[3].shape[1] == tokens and rope % 32 == 0 and (tokens + rope) % 32 == 0
        and heads_b > 0 and args[8].shape[2] == wide_l and args[9].shape[2] == wide_b
        and (args[14].shape[0] // n_sp) % 16 == 0 and (args[16].shape[1] // n_sp) % 128 == 0
    )


def solution(mesh):
    in_specs = (
        P(("sp", "tp"), None),
        P("sp", "tp", None),
        P("sp", "tp", None),
        P("sp", None),
        P("sp", None),
        P(),
        P(None, "tp", None),
        P(None, "tp", None),
        P(None, "tp", None),
        P(None, "tp", None),
        P("tp", None, None),
        P("tp", None, None),
        P(),
        P(),
        P("sp", "tp"),
        P("sp", "tp"),
        P("tp", "sp"),
    )
    out_specs = P(("sp", "tp"), None)
    grid = grid_of(mesh)

    def layer(*args):
        body = functools.partial(fused_shards, grid) if fits(grid, mesh, args) else shards
        return jax.shard_map(
            body, mesh=mesh, in_specs=in_specs, out_specs=out_specs, check_vma=False
        )(*args)

    return layer
```
